512 devices in a mesh: sp: 128 (over z, y, core), tp: 4 (over x).
Axes of the slice: x: 4, y: 8, z: 8, core: 2. Of those that a mesh axis runs over, the one named last changes fastest.
Arguments:
- glu_value: bfloat16 [131072, 1024], P('sp', 'tp'), may hold values from -6 to 6
- glu_gate: bfloat16 [131072, 1024], P('sp', 'tp'), may hold values from -8 to 8
- conv_taps: float32 [31, 1024], P(None, 'tp'), may hold values from -1 to 1
- channel_gain: float32 [1024], P('tp'), may hold values from 0.1 to 1.9
- proj_weight: bfloat16 [1024, 1024], P('tp'), may hold values from -0.1875 to 0.1875
- out_grad: bfloat16 [131072, 1024], P('sp'), may hold values from -6 to 6
Outputs:
- value_grad: bfloat16 [131072, 1024], P('sp', 'tp')
- gate_grad: bfloat16 [131072, 1024], P('sp', 'tp')
- proj_grad: float32 [1024, 1024], P(('tp', 'sp'))
- taps_grad: float32 [31, 1024], P(None, 'tp')
- norm_gain_gradient: float32 [1024], P('tp')
The draws below stay inside these ranges and needn't reach their ends.
All inputs are finite; a program needn't handle non-finite values.
Results may differ from the reference program's by a relative error of at most 0.0029.
Values may be sent and summed in bfloat16 or wider, within the bound.
No kernel may reach another device: no remote copies, remote signals or barrier semaphores. Data moves between devices by JAX's collectives and lax.ppermute only.
A program may use at most 64 MiB of HBM per device.

```python
import jax
import jax.numpy as jnp
from jax import lax

CH = 1024
KERNEL = 31
TOKENS = 131072


def levels(key, shape, split, low, high):
    def one(position, blocks):
        draws = jax.random.uniform(jax.random.fold_in(jax.random.fold_in(key, 6), position), (blocks,), jnp.float32, low / len(split), high / len(split))
        return jnp.repeat(jnp.exp(draws), shape[position] // blocks).reshape((-1,) + (1,) * (len(shape) - position - 1))

    loudness = one(*split[0])
    for cut in split[1:]:
        loudness = loudness * one(*cut)
    return loudness


def centred(stream_key, shape, spread, most, split=(), dtype=jnp.bfloat16):
    entries = spread * jax.random.normal(stream_key, shape, jnp.float32)
    if split:
        entries = entries * levels(stream_key, shape, split, -0.22, 0.18)
    return jnp.clip(entries, -most, most).astype(dtype)


def setup_inputs(seed: int = 0) -> dict:
    key_of = jax.random.split(jax.random.key(seed), 7)
    return {
        "glu_value": centred(key_of[0], (TOKENS, CH), 1.0, 6.0, ((0, 128), (1, 4))),
        "glu_gate": centred(key_of[1], (TOKENS, CH), 1.5, 8.0, ((0, 128), (1, 4))),
        "conv_taps": centred(key_of[2], (KERNEL, CH), KERNEL ** -0.5, 1.0, ((1, 4),), jnp.float32),
        "channel_gain": jnp.clip(1.0 + 0.18 * jax.random.normal(key_of[3], (CH,), jnp.float32), 0.1, 1.9),
        "proj_weight": centred(key_of[4], (CH, CH), CH ** -0.5, 0.1875, ((0, 4),)),
        "out_grad": centred(key_of[5], (TOKENS, CH), 1.0, 6.0, ((0, 128),)),
    }


def reference(glu_value, glu_gate, conv_taps, channel_gain, proj_weight, out_grad):
    halo_rows = KERNEL - 1
    row_count = glu_value.shape[0]
    value_f = glu_value.astype(jnp.float32)
    gate_sig = jax.nn.sigmoid(glu_gate.astype(jnp.float32))
    glu_out = value_f * gate_sig
    padded = jnp.pad(glu_out, ((halo_rows, 0), (0, 0)))
    convolved_output = jnp.zeros_like(glu_out)
    for tap in range(KERNEL):
        convolved_output = convolved_output + conv_taps[tap] * padded[tap:tap + row_count]
    row_average = lax.optimization_barrier(jnp.mean(convolved_output, axis=1, keepdims=True))
    row_sq = lax.optimization_barrier(jnp.mean(convolved_output * convolved_output, axis=1, keepdims=True))
    inverse_deviation = lax.rsqrt(row_sq - row_average * row_average + 1e-05)
    centered_scaled = (convolved_output - row_average) * inverse_deviation
    normalized_rows = centered_scaled * channel_gain
    activ = jax.nn.silu(normalized_rows).astype(jnp.bfloat16)
    act_grad = jnp.dot(out_grad, proj_weight.T, preferred_element_type=jnp.float32)
    norm_sig = jax.nn.sigmoid(normalized_rows)
    normalized_gradient = act_grad * norm_sig * (1.0 + normalized_rows * (1.0 - norm_sig))
    centered_scaled_gradient = normalized_gradient * channel_gain
    convolved_gradient = inverse_deviation * (centered_scaled_gradient - lax.optimization_barrier(jnp.mean(centered_scaled_gradient, axis=1, keepdims=True)) - centered_scaled * lax.optimization_barrier(jnp.mean(centered_scaled_gradient * centered_scaled, axis=1, keepdims=True)))
    gradient_factor = 1.0 / jnp.sqrt(jnp.float32(row_count))
    norm_gain_gradient = lax.optimization_barrier(jnp.sum(normalized_gradient * centered_scaled, axis=0)) * gradient_factor
    taps_grad = jnp.stack([lax.optimization_barrier(jnp.sum(convolved_gradient * padded[tap:tap + row_count], axis=0)) for tap in range(KERNEL)]) * gradient_factor
    grad_pad = jnp.pad(convolved_gradient, ((0, halo_rows), (0, 0)))
    glu_grad = jnp.zeros_like(glu_out)
    for tap in range(KERNEL):
        glu_grad = glu_grad + conv_taps[tap] * grad_pad[halo_rows - tap:halo_rows - tap + row_count]
    value_grad = (glu_grad * gate_sig).astype(jnp.bfloat16)
    gate_grad = (glu_grad * value_f * gate_sig * (1.0 - gate_sig)).astype(jnp.bfloat16)
    proj_grad = jnp.dot(activ.T, out_grad, preferred_element_type=jnp.float32) * gradient_factor
    return (value_grad, gate_grad, proj_grad, taps_grad, norm_gain_gradient)
```

```python
import jax
import jax.numpy as jnp
from jax import lax
from jax.sharding import Mesh
from jax.sharding import PartitionSpec as P

SP = ("z", "y", "core")
F32, BF16 = jnp.float32, jnp.bfloat16


def shifted(block, distance):
    devices = range(lax.axis_size(SP))
    route = [(i - distance, i) for i in devices if i - distance in devices]
    return lax.ppermute(block, SP, route)


def swapped(block):
    return lax.ppermute(block, "core", [(0, 1), (1, 0)])


def over_tp(array):
    peers = lax.axis_size("tp")
    sent = jnp.broadcast_to(array[None], (peers, *array.shape))
    return jnp.sum(lax.all_to_all(sent, "tp", 0, 0, tiled=True), axis=0)


def per_device(glu_value, glu_gate, conv_taps, channel_gain, proj_weight, out_grad):
    taps = conv_taps.shape[0]
    halo = taps - 1
    rows, width = glu_value.shape
    channels = width * lax.axis_size("tp")
    factor = 1.0 / jnp.sqrt(F32(rows * lax.axis_size(SP)))
    edge = jnp.concatenate([glu_value[rows - 32 :], glu_gate[rows - 32 :]], axis=0)
    edge = shifted(edge, 1)
    value_ext = jnp.concatenate([edge[32 - halo : 32], glu_value], axis=0)
    gate_ext = jnp.concatenate([edge[64 - halo :], glu_gate], axis=0)
    glu_out = value_ext.astype(F32) * jax.nn.sigmoid(gate_ext.astype(F32))
    conv = jnp.zeros((rows, width), F32)
    for tap in range(taps):
        conv = conv + conv_taps[tap] * glu_out[tap : tap + rows]
    sums = over_tp(jnp.stack([jnp.sum(conv, axis=1), jnp.sum(conv * conv, axis=1)]))
    mean = (sums[0] / channels)[:, None]
    rstd = lax.rsqrt((sums[1] / channels)[:, None] - mean * mean + 1e-05)
    xhat = (conv - mean) * rstd
    normed = xhat * channel_gain
    sig = jax.nn.sigmoid(normed)
    activ = (normed * sig).astype(BF16)
    act_grad = lax.dot_general(
        out_grad, proj_weight, (((1,), (1,)), ((), ())), preferred_element_type=F32
    )
    norm_grad = act_grad * sig * (1.0 + normed * (1.0 - sig))
    xhat_grad = norm_grad * channel_gain
    sums2 = over_tp(jnp.stack([jnp.sum(xhat_grad, axis=1), jnp.sum(xhat_grad * xhat, axis=1)]))
    conv_grad = rstd * (
        xhat_grad - (sums2[0] / channels)[:, None] - xhat * (sums2[1] / channels)[:, None]
    )
    z, y, i = 8, 8, 2
    me = lax.axis_index("core")
    row = lax.broadcasted_iota(jnp.int32, (width, width), 0)
    col = lax.broadcasted_iota(jnp.int32, (width, width), 1)
    half = width // 2
    source = (col % half) // i * (2 * i) + ((col // half) ^ me) * i + col % i
    order = (row == source).astype(BF16)
    activ = jnp.dot(activ, order, preferred_element_type=F32).astype(BF16)
    proj = lax.dot_general(
        activ, out_grad, (((0,), (0,)), ((), ())), preferred_element_type=F32
    )
    proj = proj[:half] + swapped(proj[half:])
    small = jnp.concatenate(
        [
            jnp.sum(conv_grad * glu_out[tap : tap + rows], axis=0)[None]
            for tap in range(taps)
        ]
        + [jnp.sum(norm_grad * xhat, axis=0)[None]],
        axis=0,
    )
    small = small + swapped(small)
    outs = channels
    first = jnp.concatenate(
        [
            proj.reshape(z, y * i, outs).astype(BF16),
            jnp.broadcast_to(
                jnp.concatenate([small[:16], small[16:]], axis=1).astype(BF16)[None], (z, 16, 512)
            ),
        ],
        axis=2,
    )
    first = jnp.sum(lax.all_to_all(first, "z", 0, 0, tiled=True).astype(F32), axis=0)
    proj = first[:, :outs].reshape(y, i * outs)
    small = first[:, outs:].reshape(1, 16 * 512)
    second = jnp.concatenate([proj, jnp.broadcast_to(small, (y, 16 * 512))], axis=1)[:, None]
    second = jnp.sum(lax.all_to_all(second, "y", 0, 0, tiled=True), axis=0)[0] * factor
    proj_grad = second[: i * outs].reshape(i, outs)
    small = second[i * outs :].reshape(16, 2, width).swapaxes(0, 1).reshape(32, width)
    taps_grad, gain_grad = small[:taps], small[taps]
    returned = shifted(conv_grad[:32], -1)
    grad_ext = jnp.concatenate([conv_grad, returned[:halo]], axis=0)
    glu_grad = jnp.zeros((rows, width), F32)
    for tap in range(taps):
        glu_grad = glu_grad + conv_taps[tap] * grad_ext[halo - tap : halo - tap + rows]
    value_f = glu_value.astype(F32)
    gate_sig = jax.nn.sigmoid(glu_gate.astype(F32))
    value_grad = (glu_grad * gate_sig).astype(BF16)
    gate_grad = (glu_grad * value_f * gate_sig * (1.0 - gate_sig)).astype(BF16)
    return (value_grad, gate_grad, proj_grad, taps_grad, gain_grad)


def solution(mesh):
    finer = Mesh(mesh.devices.reshape(8, 8, 2, mesh.shape["tp"]), (*SP, "tp"))
    return jax.shard_map(
        per_device,
        mesh=finer,
        in_specs=(P(SP, "tp"), P(SP, "tp"), P(None, "tp"), P("tp"), P("tp", None), P(SP, None)),
        out_specs=(P(SP, "tp"), P(SP, "tp"), P(("tp", *SP), None), P(None, "tp"), P("tp")),
        check_vma=False,
    )
```

```python
import math

import jax
import jax.numpy as jnp
from jax import lax
from jax.experimental import pallas as pl
from jax.experimental.pallas import tpu as pltpu
from jax.sharding import Mesh
from jax.sharding import PartitionSpec as P

SP = ("z", "y", "core")
F32, BF16 = jnp.float32, jnp.bfloat16
LANES = 128
PAD = 32
NT = (((1,), (1,)), ((), ()))
TN = (((0,), (0,)), ((), ()))


def shifted(block, distance):
    devices = range(lax.axis_size(SP))
    route = [(i - distance, i) for i in devices if i - distance in devices]
    return lax.ppermute(block, SP, route)


def swapped(block):
    return lax.ppermute(block, "core", [(0, 1), (1, 0)])


def near(array):
    return pltpu.with_memory_space_constraint(array, pltpu.VMEM)


def kernel(body, outs, args, scratch=(), aliases=None, name=None, limit=16, smem=0):
    space = pl.BlockSpec(memory_space=pltpu.VMEM)
    return pl.pallas_call(
        body,
        out_shape=[
            pltpu.VMEM(s, d) if where == "near" else jax.ShapeDtypeStruct(s, d) for s, d, where in outs
        ],
        in_specs=[pl.BlockSpec(memory_space=pltpu.SMEM)] * smem + [space] * (len(args) - smem),
        out_specs=[space] * len(outs),
        scratch_shapes=[pltpu.VMEM(s, d) for s, d in scratch],
        input_output_aliases=aliases or {},
        compiler_params=pltpu.CompilerParams(vmem_limit_bytes=limit << 20),
        name=name,
    )(*args)


def lanes(h):
    return slice(h * LANES, (h + 1) * LANES)


def glu_body(value, gate, glu, edge):
    rows = value.shape[0]

    def step(i, carry):
        r = pl.multiple_of(i * 64, 64)
        for h in range(2):
            v = value[pl.ds(r, 64), lanes(h)].astype(F32)
            g = gate[pl.ds(r, 64), lanes(h)].astype(F32)
            glu[h, pl.ds(PAD + r, 64), :] = v * jax.nn.sigmoid(g)
        return carry

    lax.fori_loop(0, rows // 64, step, 0)
    for h in range(2):
        edge[h] = glu[h, rows : rows + PAD, :]


def conv_rows(glu, taps, conv, start, count):
    n = taps.shape[0]
    for h in range(2):
        weights = [jnp.broadcast_to(taps[k : k + 1, lanes(h)], (8, LANES)) for k in range(n)]

        def step(i, carry, h=h, weights=weights):
            for u in range(2):
                r = start + i * 16 + u * 8
                parts = [None, None]
                for k in range(n):
                    term = weights[k] * glu[h, pl.ds(r + PAD + 1 - n + k, 8), :]
                    parts[k % 2] = term if parts[k % 2] is None else parts[k % 2] + term
                conv[h, pl.ds(pl.multiple_of(r, 8), 8), :] = parts[0] + parts[1]
            return carry

        lax.fori_loop(0, count // 16, step, 0)


def split(x):
    high = x.astype(BF16)
    return high, (x - high.astype(F32)).astype(BF16)


def selector(row):
    sub = lax.broadcasted_iota(jnp.int32, (8, LANES), 0)
    return (sub == row).astype(F32).astype(BF16)


def row_sums(pairs):
    total = None
    for row, x in pairs:
        pick = selector(row)
        for part in split(x):
            term = lax.dot_general(pick, part, NT, preferred_element_type=F32)
            total = term if total is None else total + term
    return total


def conv_stats(conv, stats, start, count):
    def step(i, carry):
        r = pl.multiple_of(start + i * 256, 256)
        pairs = []
        for h in range(2):
            c = conv[h, pl.ds(r, 256), :]
            pairs += [(0, c), (1, c * c)]
        stats[:, pl.ds(r, 256)] = row_sums(pairs)
        return carry

    lax.fori_loop(0, count // 256, step, 0)


def conv_body(glu, taps, conv, stats):
    rows = conv.shape[1]
    conv_rows(glu, taps, conv, 256, rows - 256)
    conv_stats(conv, stats, 256, rows - 256)


def head_body(edge, glu_in, taps, conv_in, stats_in, glu, conv, sent, stats):
    for h in range(2):
        glu[h, 0:PAD, :] = edge[h]
    conv_rows(glu, taps, conv, 0, 256)
    conv_stats(conv, stats, 0, 256)
    rows = conv.shape[1]
    for p in range(sent.shape[0]):
        sent[p, :, 0:256] = stats[0:2]
        sent[p, :, 256:rows] = stats_in[0:2, 256:rows]


def column(row):
    return jnp.broadcast_to(row, (LANES, LANES)).T


def norm_body(stats, conv, act_grad, gain, activ, xhat_out, scaled, sums, rstd_out, gain_sum, rows_in):
    peers = stats.shape[0]
    channels = 2 * LANES * peers
    total = stats[0]
    for p in range(1, peers):
        total = total + stats[p]
    mean = total[0:1] * (1.0 / channels)
    rstd = lax.rsqrt(total[1:2] * (1.0 / channels) - mean * mean + 1e-05)
    rstd_out[...] = rstd
    rows_in[0:1, :] = rstd
    rows_in[1:2, :] = mean
    for h in range(2):
        gain_sum[h] = jnp.zeros((8, LANES), F32)

    def step(i, carry):
        r = pl.multiple_of(i * LANES, LANES)
        rs = column(rows_in[0:1, pl.ds(r, LANES)])
        mu = column(rows_in[1:2, pl.ds(r, LANES)])
        pairs = []
        for h in range(2):
            g = gain[0:1, lanes(h)]
            xhat = (conv[h, pl.ds(r, LANES), :] - mu) * rs
            normed = xhat * g
            sig = jax.nn.sigmoid(normed)
            activ[pl.ds(r, LANES), lanes(h)] = (normed * sig).astype(BF16)
            ng = act_grad[pl.ds(r, LANES), lanes(h)] * (sig * (1.0 + normed * (1.0 - sig)))
            gain_sum[h] += jnp.sum((ng * xhat).reshape(16, 8, LANES), axis=0)
            xg = ng * g
            xhat_out[h, pl.ds(r, LANES), :] = xhat
            scaled[h, pl.ds(r, LANES), :] = xg * rs
            pairs += [(0, xg), (1, xg * xhat)]
        out = row_sums(pairs)
        for p in range(peers):
            sums[p, :, pl.ds(r, LANES)] = out[0:2]
        return carry

    lax.fori_loop(0, conv.shape[1] // LANES, step, 0)


def taps_body(sums, rstd, xhat, scaled, glu, gain_sum, grad, small, rows_in):
    peers = sums.shape[0]
    channels = 2 * LANES * peers
    n = small.shape[0] - 1
    rows = grad.shape[1]
    total = sums[0]
    for p in range(1, peers):
        total = total + sums[p]
    rows_in[...] = total * (rstd[...] * (1.0 / channels))

    def step(i, carry):
        r = pl.multiple_of(i * LANES, LANES)
        first = column(rows_in[0:1, pl.ds(r, LANES)])
        second = column(rows_in[1:2, pl.ds(r, LANES)])
        for h in range(2):
            at = pl.ds(r, LANES)
            grad[h, at, :] = scaled[h, at, :] - first - xhat[h, at, :] * second
        return carry

    lax.fori_loop(0, rows // LANES, step, 0)
    for h in range(2):

        def tile(i, acc, h=h):
            r = pl.multiple_of(i * 8, 8)
            c = grad[h, pl.ds(r, 8), :]
            return tuple(
                acc[k] + c * glu[h, pl.ds(r + PAD + 1 - n + k, 8), :] for k in range(n)
            )

        acc = lax.fori_loop(0, rows // 8, tile, tuple(jnp.zeros((8, LANES), F32) for _ in range(n)))
        for k in range(n):
            small[k : k + 1, lanes(h)] = jnp.sum(acc[k], axis=0, keepdims=True)
        small[n : n + 1, lanes(h)] = jnp.sum(gain_sum[h], axis=0, keepdims=True)


def pack_body(kept, received, small, other, out):
    outs = kept.shape[1]
    total = small[...] + other[...]
    low, high = total[0:16].astype(BF16), total[16:32].astype(BF16)
    for p in range(out.shape[0]):
        at = slice(p * 16, (p + 1) * 16)
        out[p, :, 0:outs] = (kept[at] + received[at]).astype(BF16)
        out[p, :, outs : outs + 256] = low
        out[p, :, outs + 256 : outs + 512] = high


def relay_body(got, out, held):
    outs = got.shape[2] - 512
    total = got[0].astype(F32)
    for p in range(1, got.shape[0]):
        total = total + got[p].astype(F32)
    held[...] = total[:, 0:outs]
    for p in range(out.shape[0]):
        out[p, :, 0:512] = total[0:8, outs:]
        out[p, :, 512:1024] = total[8:16, outs:]
        for i in range(2):
            for j in range(4):
                out[p, 4 * i + j : 4 * i + j + 1, 1024:1280] = held[
                    2 * p + i : 2 * p + i + 1, 256 * j : 256 * j + 256
                ]


def final_body(factor, got, proj, taps, gain):
    total = got[0]
    for p in range(1, got.shape[0]):
        total = total + got[p]
    total = total * factor
    taps[0:8] = total[:, 0:256]
    taps[16:24] = total[:, 256:512]
    taps[8:16] = total[:, 512:768]
    taps[24:31] = total[0:7, 768:1024]
    gain[...] = total[7:8, 768:1024]
    for i in range(2):
        for j in range(4):
            proj[i : i + 1, 256 * j : 256 * j + 256] = total[4 * i + j : 4 * i + j + 1, 1024:1280]


def glu_grad_body(grad, after, taps, value, gate, value_grad, gate_grad, ext):
    rows = grad.shape[1]
    n = taps.shape[0]

    def fill(i, carry):
        r = pl.multiple_of(i * 64, 64)
        for h in range(2):
            ext[h, pl.ds(r, 64), :] = grad[h, pl.ds(r, 64), :]
        return carry

    lax.fori_loop(0, rows // 64, fill, 0)
    for h in range(2):
        ext[h, rows : rows + PAD, :] = after[h]
        weights = [jnp.broadcast_to(taps[k : k + 1, lanes(h)], (8, LANES)) for k in range(n)]

        def step(i, carry, h=h, weights=weights):
            tiles = []
            for u in range(2):
                r = i * 16 + u * 8
                parts = [None, None]
                for k in range(n):
                    term = weights[k] * ext[h, pl.ds(r + n - 1 - k, 8), :]
                    parts[k % 2] = term if parts[k % 2] is None else parts[k % 2] + term
                tiles.append(parts[0] + parts[1])
            at = pl.ds(pl.multiple_of(i * 16, 16), 16)
            dglu = jnp.concatenate(tiles, axis=0)
            sig = jax.nn.sigmoid(gate[at, lanes(h)].astype(F32))
            got = dglu * sig
            value_grad[at, lanes(h)] = got.astype(BF16)
            gate_grad[at, lanes(h)] = (got * value[at, lanes(h)].astype(F32) * (1.0 - sig)).astype(BF16)
            return carry

        lax.fori_loop(0, rows // 16, step, 0)


def act_body(out_grad, weight, act):
    act[...] = lax.dot_general(out_grad[...], weight[...], NT, preferred_element_type=F32)


def proj_body(me, activ, out_grad, kept, sent):
    width = activ.shape[1]
    half, i = width // 2, 2
    row = lax.broadcasted_iota(jnp.int32, (width, width), 0)
    col = lax.broadcasted_iota(jnp.int32, (width, width), 1)
    low = jnp.bitwise_and(col, half - 1)
    high = jnp.bitwise_xor(jnp.right_shift(col, 7), me[0])
    source = jnp.left_shift(jnp.right_shift(low, 1), 2) + 2 * high + jnp.bitwise_and(col, 1)
    order = (row == source).astype(F32).astype(BF16)
    placed = jnp.dot(activ[...], order, preferred_element_type=F32).astype(BF16)
    kept[...] = lax.dot_general(placed[:, :half], out_grad[...], TN, preferred_element_type=F32)
    sent[...] = lax.dot_general(placed[:, half:], out_grad[...], TN, preferred_element_type=F32)


def over_tp(array):
    return lax.all_to_all(array, "tp", 0, 0, tiled=True)


def per_device(glu_value, glu_gate, conv_taps, channel_gain, proj_weight, out_grad):
    n = conv_taps.shape[0]
    rows, width = glu_value.shape
    peers = lax.axis_size("tp")
    outs = out_grad.shape[1]
    factor = 1.0 / math.sqrt(rows * lax.axis_size(SP))
    def wide(length):
        return ((2, length, LANES), F32, "near")

    stat = ((peers, 2, rows), F32, "far")
    glu, edge = kernel(glu_body, [wide(rows + PAD), wide(PAD)], (glu_value, glu_gate), name="glu")
    edge = shifted(edge, 1)
    conv, stats = kernel(
        conv_body, [wide(rows), ((8, rows), F32, "near")], (near(glu), conv_taps), name="conv"
    )
    glu, conv, stats = kernel(
        head_body,
        [wide(rows + PAD), wide(rows), stat],
        (near(edge), near(glu), conv_taps, near(conv), near(stats)),
        aliases={1: 0, 3: 1},
        scratch=[((8, 256), F32)],
        name="head",
    )
    stats = over_tp(stats)
    (act_grad,) = kernel(
        act_body, [((rows, width), F32, "near")], (out_grad, proj_weight), name="act"
    )
    stats, act_grad = lax.optimization_barrier((stats, act_grad))
    activ, xhat, scaled, sums, rstd, gain_sum = kernel(
        norm_body,
        [
            ((rows, width), BF16, "near"),
            wide(rows),
            wide(rows),
            stat,
            ((1, rows), F32, "near"),
            wide(8),
        ],
        (near(stats), near(conv), near(act_grad), channel_gain[None]),
        scratch=[((2, rows), F32)],
        name="norm",
    )
    sums = over_tp(sums)
    kept, sent = kernel(
        proj_body,
        [((width // 2, outs), F32, "near")] * 2,
        (lax.axis_index("core")[None], activ, out_grad),
        name="proj",
        smem=1,
    )
    sums, sent = lax.optimization_barrier((sums, sent))
    received = swapped(sent)
    grad, small = kernel(
        taps_body,
        [wide(rows), ((n + 1, width), F32, "near")],
        (near(sums), near(rstd), near(xhat), near(scaled), near(glu), near(gain_sum)),
        scratch=[((2, rows), F32)],
        name="taps",
    )
    other = swapped(small)
    (first,) = kernel(
        pack_body,
        [((8, 16, outs + 512), BF16, "far")],
        (near(kept), near(received), near(small), near(other)),
        name="pack",
    )
    first = lax.all_to_all(first, "z", 0, 0, tiled=True)
    after = shifted(grad[:, :PAD], -1)
    first, after = lax.optimization_barrier((first, after))
    (second,) = kernel(
        relay_body,
        [((8, 8, 1280), F32, "far")],
        (near(first),),
        scratch=[((16, outs), F32)],
        name="relay",
    )
    second = lax.all_to_all(second, "y", 0, 0, tiled=True)
    value_grad, gate_grad = kernel(
        glu_grad_body,
        [((rows, width), BF16, "far")] * 2,
        (near(grad), near(after), conv_taps, glu_value, glu_gate),
        scratch=[((2, rows + PAD, LANES), F32)],
        name="glu_grad",
    )
    second, value_grad, gate_grad = lax.optimization_barrier((second, value_grad, gate_grad))
    proj_grad, taps_grad, gain_grad = kernel(
        lambda *refs: final_body(factor, *refs),
        [((2, outs), F32, "far"), ((n, width), F32, "far"), ((1, width), F32, "far")],
        (near(second),),
        name="final",
    )
    return (value_grad, gate_grad, proj_grad, taps_grad, gain_grad.reshape(width))


def solution(mesh):
    finer = Mesh(mesh.devices.reshape(8, 8, 2, mesh.shape["tp"]), (*SP, "tp"))
    return jax.shard_map(
        per_device,
        mesh=finer,
        in_specs=(P(SP, "tp"), P(SP, "tp"), P(None, "tp"), P("tp"), P("tp", None), P(SP, None)),
        out_specs=(P(SP, "tp"), P(SP, "tp"), P(("tp", *SP), None), P(None, "tp"), P("tp")),
        check_vma=False,
    )
```

```python
import math

import jax
import jax.numpy as jnp
from jax import lax
from jax.experimental import pallas as pl
from jax.experimental.pallas import tpu as pltpu
from jax.sharding import Mesh
from jax.sharding import PartitionSpec as P


SP = ("z", "y", "core")
F32, BF16 = jnp.float32, jnp.bfloat16
LANES = 128
PAD = 32
NT = (((1,), (1,)), ((), ()))
TN = (((0,), (0,)), ((), ()))


def shifted(block, distance):
    devices = range(lax.axis_size(SP))
    route = [(i - distance, i) for i in devices if i - distance in devices]
    return lax.ppermute(block, SP, route)


def swapped(block):
    return lax.ppermute(block, "core", [(0, 1), (1, 0)])


def near(array):
    return pltpu.with_memory_space_constraint(array, pltpu.VMEM)


def far(array):
    return pltpu.with_memory_space_constraint(array, pltpu.HBM)


VMEM, HBM, SMEM = (pl.BlockSpec(memory_space=m) for m in (pltpu.VMEM, pltpu.HBM, pltpu.SMEM))


def kernel(body, outs, args, ins=(), out_specs=None, scratch=(), aliases=None, limit=16):
    shapes = {
        "near": pltpu.VMEM,
        "far": pltpu.HBM,
        "any": jax.ShapeDtypeStruct,
    }
    return pl.pallas_call(
        body,
        out_shape=[shapes[where](s, d) for s, d, where in outs],
        in_specs=list(ins) + [VMEM] * (len(args) - len(ins)),
        out_specs=out_specs or [VMEM] * len(outs),
        scratch_shapes=[pltpu.VMEM(*x) if isinstance(x, tuple) else x for x in scratch],
        input_output_aliases=aliases or {},
        compiler_params=pltpu.CompilerParams(vmem_limit_bytes=limit << 20),
    )(*args)


def lanes(h):
    return slice(h * LANES, (h + 1) * LANES)


def glu_body(value_in, gate_in, taps_in, glu, edge, taps, value, gate, sems):
    rows = value.shape[0]
    chunks = sems.shape[1] - 1
    size = rows // chunks
    load_taps = pltpu.make_async_copy(taps_in, taps, sems.at[0, chunks])
    loads = []
    for c in range(chunks):
        at = pl.ds(c * size, size)
        loads.append(pltpu.make_async_copy(value_in.at[at], value.at[at], sems.at[0, c]))
        loads.append(pltpu.make_async_copy(gate_in.at[at], gate.at[at], sems.at[1, c]))
    for load in loads:
        load.start()
    load_taps.start()
    for c in range(chunks):
        loads[2 * c].wait()
        loads[2 * c + 1].wait()

        def step(i, carry, c=c):
            r = pl.multiple_of(c * size + i * 64, 64)
            for h in range(2):
                v = value[pl.ds(r, 64), lanes(h)].astype(F32)
                g = gate[pl.ds(r, 64), lanes(h)].astype(F32)
                glu[h, pl.ds(PAD + r, 64), :] = v * jax.nn.sigmoid(g)
            return carry

        lax.fori_loop(0, size // 64, step, 0)
    for h in range(2):
        edge[h] = glu[h, rows : rows + PAD, :]
    load_taps.wait()


def conv_rows(glu, taps, conv, start, count):
    n = taps.shape[0]
    for h in range(2):
        weights = [jnp.broadcast_to(taps[k : k + 1, lanes(h)], (8, LANES)) for k in range(n)]

        def step(i, carry, h=h, weights=weights):
            for u in range(4):
                r = start + i * 32 + u * 8
                parts = [None, None]
                for k in range(n):
                    term = weights[k] * glu[h, pl.ds(r + PAD + 1 - n + k, 8), :]
                    parts[k % 2] = term if parts[k % 2] is None else parts[k % 2] + term
                conv[h, pl.ds(pl.multiple_of(r, 8), 8), :] = parts[0] + parts[1]
            return carry

        lax.fori_loop(0, count // 32, step, 0)


def split(x):
    high = x.astype(BF16)
    return high, (x - high.astype(F32)).astype(BF16)


def selector(row):
    sub = lax.broadcasted_iota(jnp.int32, (8, LANES), 0)
    return (sub == row).astype(F32).astype(BF16)


def row_sums(pairs):
    total = None
    for row, x in pairs:
        pick = selector(row)
        for part in split(x):
            term = lax.dot_general(pick, part, NT, preferred_element_type=F32)
            total = term if total is None else total + term
    return total


def conv_stats(conv, stats, start, count):
    def step(i, carry):
        r = pl.multiple_of(start + i * 256, 256)
        pairs = []
        for h in range(2):
            c = conv[h, pl.ds(r, 256), :]
            pairs += [(0, c), (1, c * c)]
        stats[:, pl.ds(r, 256)] = row_sums(pairs)
        return carry

    lax.fori_loop(0, count // 256, step, 0)


def conv_body(glu, taps, conv, stats, saved, sem):
    rows = conv.shape[1]
    store = pltpu.make_async_copy(
        glu.at[:, pl.ds(PAD, rows)], saved.at[:, pl.ds(PAD, rows)], sem
    )
    store.start()
    conv_rows(glu, taps, conv, 256, rows - 256)
    conv_stats(conv, stats, 256, rows - 256)
    store.wait()


def head_body(saved_in, edge, glu_in, taps, conv_in, stats_in, saved, glu, conv, sent, stats, sem):
    store = pltpu.make_async_copy(edge, saved.at[:, pl.ds(0, PAD)], sem)
    store.start()
    for h in range(2):
        glu[h, 0:PAD, :] = edge[h]
    conv_rows(glu, taps, conv, 0, 256)
    conv_stats(conv, stats, 0, 256)
    rows = conv.shape[1]
    for p in range(sent.shape[0]):
        sent[p, :, 0:256] = stats[0:2]
        sent[p, :, 256:rows] = stats_in[0:2, 256:rows]
    store.wait()


def column(row):
    return jnp.broadcast_to(row, (LANES, LANES)).T


def norm_body(
    stats, conv, act_grad, gain, activ_out, xhat_out, scaled, sums, rstd_out, gain_sum,
    rows_in, activ, xhats, sems,
):
    peers = stats.shape[0]
    channels = 2 * LANES * peers
    total = stats[0]
    for p in range(1, peers):
        total = total + stats[p]
    mean = total[0:1] * (1.0 / channels)
    rstd = lax.rsqrt(total[1:2] * (1.0 / channels) - mean * mean + 1e-05)
    rstd_out[...] = rstd
    rows_in[0:1, :] = rstd
    rows_in[1:2, :] = mean
    for h in range(2):
        gain_sum[h] = jnp.zeros((8, LANES), F32)

    def store(i):
        at = pl.ds(pl.multiple_of(i * LANES, LANES), LANES)
        return (
            pltpu.make_async_copy(activ.at[at], activ_out.at[at], sems.at[0, i]),
            pltpu.make_async_copy(xhats.at[:, at], xhat_out.at[:, at], sems.at[1, i]),
        )

    def step(i, carry):
        r = pl.multiple_of(i * LANES, LANES)
        rs = column(rows_in[0:1, pl.ds(r, LANES)])
        mu = column(rows_in[1:2, pl.ds(r, LANES)])
        pairs = []
        for h in range(2):
            g = gain[0:1, lanes(h)]
            xhat = (conv[h, pl.ds(r, LANES), :] - mu) * rs
            normed = xhat * g
            sig = jax.nn.sigmoid(normed)
            activ[pl.ds(r, LANES), lanes(h)] = (normed * sig).astype(BF16)
            ng = act_grad[pl.ds(r, LANES), lanes(h)] * (sig * (1.0 + normed * (1.0 - sig)))
            gain_sum[h] += jnp.sum((ng * xhat).reshape(16, 8, LANES), axis=0)
            xg = ng * g
            xhats[h, pl.ds(r, LANES), :] = xhat
            scaled[h, pl.ds(r, LANES), :] = xg * rs
            pairs += [(0, xg), (1, xg * xhat)]
        out = row_sums(pairs)
        for p in range(peers):
            sums[p, :, pl.ds(r, LANES)] = out[0:2]
        for copy in store(i):
            copy.start()
        return carry

    blocks = conv.shape[1] // LANES
    lax.fori_loop(0, blocks, step, 0)
    for i in range(blocks):
        for copy in store(i):
            copy.wait()


def taps_body(
    kept_in, xhat_in, glu_in, received, sums, rstd, scaled, gain_sum, grad, small, packed,
    rows_in, columns, kept, xhat, glu, joined, sems,
):
    rows = grad.shape[1]
    load_xhat = pltpu.make_async_copy(xhat_in, xhat, sems.at[0])
    load_kept = pltpu.make_async_copy(kept_in, kept, sems.at[1])
    load_glu = pltpu.make_async_copy(glu_in, glu, sems.at[2])
    load_xhat.start()
    load_kept.start()
    load_glu.start()
    peers = sums.shape[0]
    channels = 2 * LANES * peers
    n = small.shape[0] - 1
    total = sums[0]
    for p in range(1, peers):
        total = total + sums[p]
    rows_in[...] = total * (rstd[...] * (1.0 / channels))
    for b in range(rows // LANES):
        at = slice(b * LANES, (b + 1) * LANES)
        columns[0, at] = column(rows_in[0:1, at])
        columns[1, at] = column(rows_in[1:2, at])
    load_xhat.wait()

    def step(i, carry):
        at = pl.ds(pl.multiple_of(i * 64, 64), 64)
        for h in range(2):
            grad[h, at, :] = scaled[h, at, :] - columns[0, at] - xhat[h, at, :] * columns[1, at]
        return carry

    lax.fori_loop(0, rows // 64, step, 0)
    load_kept.wait()
    for p in range(joined.shape[0]):
        at = slice(p * 16, (p + 1) * 16)
        joined[p] = (kept[at] + received[at]).astype(BF16)
    store = pltpu.make_async_copy(joined, packed.at[:, :, pl.ds(0, joined.shape[2])], sems.at[3])
    store.start()
    load_glu.wait()
    for h in range(2):
        for lo, hi in ((0, 16), (16, n)):

            def tile(i, acc, h=h, lo=lo, hi=hi):
                acc = list(acc)
                for u in range(4):
                    r = pl.multiple_of(i * 32 + u * 8, 8)
                    c = grad[h, pl.ds(r, 8), :]
                    for k in range(lo, hi):
                        acc[k - lo] = acc[k - lo] + c * glu[h, pl.ds(r + PAD + 1 - n + k, 8), :]
                return tuple(acc)

            zero = tuple(jnp.zeros((8, LANES), F32) for _ in range(lo, hi))
            acc = lax.fori_loop(0, rows // 32, tile, zero)
            for k in range(lo, hi):
                small[k : k + 1, lanes(h)] = jnp.sum(acc[k - lo], axis=0, keepdims=True)
        small[n : n + 1, lanes(h)] = jnp.sum(gain_sum[h], axis=0, keepdims=True)
    store.wait()


def pack_body(packed_in, small, other, packed, piece, sem):
    total = small[...] + other[...]
    low, high = total[0:16].astype(BF16), total[16:32].astype(BF16)
    for p in range(piece.shape[0]):
        piece[p, :, 0:256] = low
        piece[p, :, 256:512] = high
    outs = packed.shape[2] - 512
    store = pltpu.make_async_copy(piece, packed.at[:, :, pl.ds(outs, 512)], sem)
    store.start()
    store.wait()


def relay_body(got, out, held):
    outs = got.shape[2] - 512
    total = got[0].astype(F32)
    for p in range(1, got.shape[0]):
        total = total + got[p].astype(F32)
    held[...] = total[:, 0:outs]
    for p in range(out.shape[0]):
        out[p, :, 0:512] = total[0:8, outs:]
        out[p, :, 512:1024] = total[8:16, outs:]
        for i in range(2):
            for j in range(4):
                out[p, 4 * i + j : 4 * i + j + 1, 1024:1280] = held[
                    2 * p + i : 2 * p + i + 1, 256 * j : 256 * j + 256
                ]


def final_body(factor, got, proj, taps, gain):
    total = got[0]
    for p in range(1, got.shape[0]):
        total = total + got[p]
    total = total * factor
    taps[0:8] = total[:, 0:256]
    taps[16:24] = total[:, 256:512]
    taps[8:16] = total[:, 512:768]
    taps[24:31] = total[0:7, 768:1024]
    gain[...] = total[7:8, 768:1024]
    for i in range(2):
        for j in range(4):
            proj[i : i + 1, 256 * j : 256 * j + 256] = total[4 * i + j : 4 * i + j + 1, 1024:1280]


def glu_grad_body(grad, after, taps, value, gate, value_grad, gate_grad, ext):
    rows = grad.shape[1]
    n = taps.shape[0]

    def fill(i, carry):
        r = pl.multiple_of(i * 64, 64)
        for h in range(2):
            ext[h, pl.ds(r, 64), :] = grad[h, pl.ds(r, 64), :]
        return carry

    lax.fori_loop(0, rows // 64, fill, 0)
    for h in range(2):
        ext[h, rows : rows + PAD, :] = after[h]
        weights = [jnp.broadcast_to(taps[k : k + 1, lanes(h)], (8, LANES)) for k in range(n)]

        def step(i, carry, h=h, weights=weights):
            tiles = []
            for u in range(2):
                r = i * 16 + u * 8
                parts = [None, None]
                for k in range(n):
                    term = weights[k] * ext[h, pl.ds(r + n - 1 - k, 8), :]
                    parts[k % 2] = term if parts[k % 2] is None else parts[k % 2] + term
                tiles.append(parts[0] + parts[1])
            at = pl.ds(pl.multiple_of(i * 16, 16), 16)
            dglu = jnp.concatenate(tiles, axis=0)
            sig = jax.nn.sigmoid(gate[at, lanes(h)].astype(F32))
            got = dglu * sig
            value_grad[at, lanes(h)] = got.astype(BF16)
            gate_grad[at, lanes(h)] = (got * value[at, lanes(h)].astype(F32) * (1.0 - sig)).astype(BF16)
            return carry

        lax.fori_loop(0, rows // 16, step, 0)


def act_body(grad_in, weight_in, act, out_grad, weight, sems):
    rows = out_grad.shape[0]
    size = rows // 4
    load_weight = pltpu.make_async_copy(weight_in, weight, sems.at[4])
    load_weight.start()
    loads = []
    for c in range(4):
        at = pl.ds(c * size, size)
        loads.append(pltpu.make_async_copy(grad_in.at[at], out_grad.at[at], sems.at[c]))
        loads[c].start()
    load_weight.wait()
    for c in range(4):
        loads[c].wait()
        at = pl.ds(c * size, size)
        act[at] = lax.dot_general(out_grad[at], weight[...], NT, preferred_element_type=F32)


def proj_body(me, activ_in, grad_in, kept, sent, activ, out_grad, sems):
    load_activ = pltpu.make_async_copy(activ_in, activ, sems.at[0])
    load_grad = pltpu.make_async_copy(grad_in, out_grad, sems.at[1])
    load_activ.start()
    load_grad.start()
    width = activ.shape[1]
    half = width // 2
    row = lax.broadcasted_iota(jnp.int32, (width, width), 0)
    col = lax.broadcasted_iota(jnp.int32, (width, width), 1)
    low = jnp.bitwise_and(col, half - 1)
    high = jnp.bitwise_xor(jnp.right_shift(col, 7), me[0])
    source = jnp.left_shift(jnp.right_shift(low, 1), 2) + 2 * high + jnp.bitwise_and(col, 1)
    order = (row == source).astype(F32).astype(BF16)
    load_activ.wait()
    placed = jnp.dot(activ[...], order, preferred_element_type=F32).astype(BF16)
    load_grad.wait()
    sent[...] = lax.dot_general(placed[:, half:], out_grad[...], TN, preferred_element_type=F32)
    kept[...] = lax.dot_general(placed[:, :half], out_grad[...], TN, preferred_element_type=F32)


def over_tp(array):
    return lax.all_to_all(array, "tp", 0, 0, tiled=True)


def per_device(glu_value, glu_gate, conv_taps, channel_gain, proj_weight, out_grad):
    n = conv_taps.shape[0]
    rows, width = glu_value.shape
    peers = lax.axis_size("tp")
    outs = out_grad.shape[1]
    factor = 1.0 / math.sqrt(rows * lax.axis_size(SP))

    def wide(length):
        return ((2, length, LANES), F32, "near")

    def kept_wide(length):
        return ((2, length, LANES), F32, "far")

    stat = ((peers, 2, rows), F32, "any")
    dma = pltpu.SemaphoreType.DMA
    tall = ((rows, width), BF16)
    glu, edge, taps = kernel(
        glu_body,
        [wide(rows + PAD), wide(PAD), ((n, width), F32, "near")],
        (far(glu_value), far(glu_gate), far(conv_taps)),
        ins=[HBM] * 3,
        scratch=[tall, tall, dma((2, 5))],
    )
    edge = shifted(edge, 1)
    conv, stats, saved = kernel(
        conv_body,
        [wide(rows), ((8, rows), F32, "near"), kept_wide(rows + PAD)],
        (near(glu), near(taps)),
        out_specs=[VMEM, VMEM, HBM],
        scratch=[dma],
    )
    saved, _, conv, stats = kernel(
        head_body,
        [kept_wide(rows + PAD), wide(rows + PAD), wide(rows), stat],
        (far(saved), near(edge), near(glu), near(taps), near(conv), near(stats)),
        ins=[HBM],
        out_specs=[HBM, VMEM, VMEM, VMEM],
        aliases={0: 0, 2: 1, 4: 2},
        scratch=[((8, 256), F32), dma],
    )
    stats = over_tp(stats)
    (act_grad,) = kernel(
        act_body,
        [((rows, width), F32, "near")],
        (far(out_grad), far(proj_weight)),
        ins=[HBM] * 2,
        scratch=[((rows, outs), BF16), ((width, outs), BF16), dma((5,))],
    )
    stats, act_grad = lax.optimization_barrier((stats, act_grad))
    activ, xhat, scaled, sums, rstd, gain_sum = kernel(
        norm_body,
        [
            (*tall, "far"),
            kept_wide(rows),
            wide(rows),
            stat,
            ((1, rows), F32, "near"),
            wide(8),
        ],
        (near(stats), near(conv), near(act_grad), channel_gain[None]),
        out_specs=[HBM] * 2 + [VMEM] * 4,
        scratch=[((2, rows), F32), tall, wide(rows)[:2], dma((2, rows // LANES))],
    )
    sums = over_tp(sums)
    kept, sent = kernel(
        proj_body,
        [((width // 2, outs), F32, "far")] * 2,
        (lax.axis_index("core")[None], far(activ), far(out_grad)),
        ins=[SMEM, HBM, HBM],
        scratch=[tall, ((rows, outs), BF16), dma((2,))],
    )
    received = swapped(sent)
    sums, received = lax.optimization_barrier((sums, received))
    payload = ((8, 16, outs + 512), BF16, "far")
    share = ((width // 2, outs), F32)
    grad, small, first = kernel(
        taps_body,
        [wide(rows), ((n + 1, width), F32, "near"), payload],
        (
            far(kept), far(xhat), far(saved), near(received), near(sums), near(rstd),
            near(scaled), near(gain_sum),
        ),
        ins=[HBM] * 3,
        out_specs=[VMEM, VMEM, HBM],
        scratch=[
            ((2, rows), F32),
            ((2, rows, LANES), F32),
            share,
            wide(rows)[:2],
            wide(rows + PAD)[:2],
            ((8, 16, outs), BF16),
            dma((4,)),
        ],
    )
    other = swapped(small)
    (first,) = kernel(
        pack_body,
        [payload],
        (far(first), near(small), near(other)),
        ins=[HBM],
        out_specs=[HBM],
        aliases={0: 0},
        scratch=[((8, 16, 512), BF16), dma],
    )
    first = lax.all_to_all(first, "z", 0, 0, tiled=True)
    after = shifted(grad[:, :PAD], -1)
    first, after = lax.optimization_barrier((first, after))
    (second,) = kernel(
        relay_body, [((8, 8, 1280), F32, "any")], (near(first),), scratch=[((16, outs), F32)]
    )
    second = lax.all_to_all(second, "y", 0, 0, tiled=True)
    value_grad, gate_grad = kernel(
        glu_grad_body,
        [((rows, width), BF16, "any")] * 2,
        (near(grad), near(after), conv_taps, glu_value, glu_gate),
        scratch=[((2, rows + PAD, LANES), F32)],
    )
    second, value_grad, gate_grad = lax.optimization_barrier((second, value_grad, gate_grad))
    proj_grad, taps_grad, gain_grad = kernel(
        lambda *refs: final_body(factor, *refs),
        [((2, outs), F32, "any"), ((n, width), F32, "any"), ((1, width), F32, "any")],
        (near(second),),
    )
    return (value_grad, gate_grad, proj_grad, taps_grad, gain_grad.reshape(width))


def solution(mesh):
    finer = Mesh(mesh.devices.reshape(8, 8, 2, mesh.shape["tp"]), (*SP, "tp"))
    return jax.shard_map(
        per_device,
        mesh=finer,
        in_specs=(P(SP, "tp"), P(SP, "tp"), P(None, "tp"), P("tp"), P("tp", None), P(SP, None)),
        out_specs=(P(SP, "tp"), P(SP, "tp"), P(("tp", *SP), None), P(None, "tp"), P("tp")),
        check_vma=False,
    )
```

```python
import math

import jax
import jax.numpy as jnp
from jax import lax
from jax.experimental import pallas as pl
from jax.experimental.pallas import tpu as pltpu
from jax.sharding import Mesh
from jax.sharding import PartitionSpec as P


SP = ("z", "y", "core")
F32, BF16 = jnp.float32, jnp.bfloat16
LANES = 128
PAD = 32
NT = (((1,), (1,)), ((), ()))


def shifted(block, distance):
    devices = range(lax.axis_size(SP))
    route = [(i - distance, i) for i in devices if i - distance in devices]
    return lax.ppermute(block, SP, route)


def swapped(block):
    return lax.ppermute(block, "core", [(0, 1), (1, 0)])


def near(array):
    return pltpu.with_memory_space_constraint(array, pltpu.VMEM)


def far(array):
    return pltpu.with_memory_space_constraint(array, pltpu.HBM)


VMEM, HBM, SMEM = (pl.BlockSpec(memory_space=m) for m in (pltpu.VMEM, pltpu.HBM, pltpu.SMEM))


def kernel(body, outs, args, ins=(), out_specs=None, scratch=(), aliases=None, limit=16):
    shapes = {
        "near": pltpu.VMEM,
        "far": pltpu.HBM,
        "any": jax.ShapeDtypeStruct,
    }
    return pl.pallas_call(
        body,
        out_shape=[shapes[where](s, d) for s, d, where in outs],
        in_specs=list(ins) + [VMEM] * (len(args) - len(ins)),
        out_specs=out_specs or [VMEM] * len(outs),
        scratch_shapes=[pltpu.VMEM(*x) if isinstance(x, tuple) else x for x in scratch],
        input_output_aliases=aliases or {},
        compiler_params=pltpu.CompilerParams(vmem_limit_bytes=limit << 20),
    )(*args)


def lanes(h):
    return slice(h * LANES, (h + 1) * LANES)


def glu_body(value_in, gate_in, taps_in, glu, edge, taps, value, gate, sems):
    rows = value.shape[0]
    chunks = sems.shape[1] - 1
    size = rows // chunks
    load_taps = pltpu.make_async_copy(taps_in, taps, sems.at[0, chunks])
    loads = []
    for c in range(chunks):
        at = pl.ds(c * size, size)
        loads.append(pltpu.make_async_copy(value_in.at[at], value.at[at], sems.at[0, c]))
        loads.append(pltpu.make_async_copy(gate_in.at[at], gate.at[at], sems.at[1, c]))
    for load in loads:
        load.start()
    load_taps.start()
    for c in range(chunks):
        loads[2 * c].wait()
        loads[2 * c + 1].wait()

        def step(i, carry, c=c):
            r = pl.multiple_of(c * size + i * 64, 64)
            for h in range(2):
                v = value[pl.ds(r, 64), lanes(h)].astype(F32)
                g = gate[pl.ds(r, 64), lanes(h)].astype(F32)
                glu[h, pl.ds(PAD + r, 64), :] = v * jax.nn.sigmoid(g)
            return carry

        lax.fori_loop(0, size // 64, step, 0)
    for h in range(2):
        edge[h] = glu[h, rows : rows + PAD, :]
    load_taps.wait()


def conv_rows(glu, taps, conv, start, count):
    n = taps.shape[0]
    for h in range(2):
        weights = [jnp.broadcast_to(taps[k : k + 1, lanes(h)], (8, LANES)) for k in range(n)]

        def step(i, carry, h=h, weights=weights):
            for u in range(4):
                r = start + i * 32 + u * 8
                parts = [None, None]
                for k in range(n):
                    term = weights[k] * glu[h, pl.ds(r + PAD + 1 - n + k, 8), :]
                    parts[k % 2] = term if parts[k % 2] is None else parts[k % 2] + term
                conv[h, pl.ds(pl.multiple_of(r, 8), 8), :] = parts[0] + parts[1]
            return carry

        lax.fori_loop(0, count // 32, step, 0)


def split(x):
    high = x.astype(BF16)
    return high, (x - high.astype(F32)).astype(BF16)


def selector(row):
    sub = lax.broadcasted_iota(jnp.int32, (8, LANES), 0)
    return (sub == row).astype(F32).astype(BF16)


def row_sums(pairs):
    total = None
    for row, x in pairs:
        pick = selector(row)
        for part in split(x):
            term = lax.dot_general(pick, part, NT, preferred_element_type=F32)
            total = term if total is None else total + term
    return total


def conv_stats(conv, stats, start, count):
    def step(i, carry):
        r = pl.multiple_of(start + i * 256, 256)
        pairs = []
        for h in range(2):
            c = conv[h, pl.ds(r, 256), :]
            pairs += [(0, c), (1, c * c)]
        stats[:, pl.ds(r, 256)] = row_sums(pairs)
        return carry

    lax.fori_loop(0, count // 256, step, 0)


def conv_body(glu, taps, conv, stats, saved, sem):
    rows = conv.shape[1]
    store = pltpu.make_async_copy(
        glu.at[:, pl.ds(PAD, rows)], saved.at[:, pl.ds(PAD, rows)], sem
    )
    store.start()
    conv_rows(glu, taps, conv, 256, rows - 256)
    conv_stats(conv, stats, 256, rows - 256)
    store.wait()


def head_body(saved_in, edge, glu_in, taps, conv_in, stats_in, saved, glu, conv, sent, stats, sem):
    store = pltpu.make_async_copy(edge, saved.at[:, pl.ds(0, PAD)], sem)
    store.start()
    for h in range(2):
        glu[h, 0:PAD, :] = edge[h]
    conv_rows(glu, taps, conv, 0, 256)
    conv_stats(conv, stats, 0, 256)
    rows = conv.shape[1]
    for p in range(sent.shape[0]):
        sent[p, :, 0:256] = stats[0:2]
        sent[p, :, 256:rows] = stats_in[0:2, 256:rows]
    store.wait()


def spread(rows, stack, columns):
    stats, length = rows.shape
    blocks = length // LANES
    stack[...] = jnp.zeros(stack.shape, F32)
    for s in range(stats):
        for b in range(blocks):
            stack[s * blocks + b : s * blocks + b + 1, :] = rows[s : s + 1, b * LANES : (b + 1) * LANES]
    turned = stack[...].T
    for s in range(stats):
        for b in range(blocks):
            j = s * blocks + b
            columns[s, b * LANES : (b + 1) * LANES] = jnp.broadcast_to(
                turned[:, j : j + 1], (LANES, LANES)
            )


def norm_body(
    stats, conv, act_grad, gain, activ_out, xhat_out, scaled, sums, gain_sum,
    rows_in, stack, columns, activ, xhats, sems,
):
    peers = stats.shape[0]
    rows = conv.shape[1]
    channels = 2 * LANES * peers
    total = stats[0]
    for p in range(1, peers):
        total = total + stats[p]
    mean = total[0:1] * (1.0 / channels)
    rows_in[0:1, :] = lax.rsqrt(total[1:2] * (1.0 / channels) - mean * mean + 1e-05)
    rows_in[1:2, :] = mean
    spread(rows_in, stack, columns)
    for h in range(2):
        gain_sum[h] = jnp.zeros((8, LANES), F32)
    size = 256

    def store(i):
        at = pl.ds(pl.multiple_of(i * size, size), size)
        return (
            pltpu.make_async_copy(activ.at[at], activ_out.at[at], sems.at[0, i]),
            pltpu.make_async_copy(xhats.at[:, at], xhat_out.at[:, at], sems.at[1, i]),
        )

    def block(i, carry):
        def step(j, carry):
            at = pl.ds(pl.multiple_of(i * size + j * 32, 32), 32)
            rs, mu = columns[0, at], columns[1, at]
            for h in range(2):
                g = gain[0:1, lanes(h)]
                xhat = (conv[h, at, :] - mu) * rs
                normed = xhat * g
                sig = jax.nn.sigmoid(normed)
                act = normed * sig
                activ[at, lanes(h)] = act.astype(BF16)
                ng = act_grad[at, lanes(h)] * (sig + act * (1.0 - sig))
                gain_sum[h] += jnp.sum((ng * xhat).reshape(4, 8, LANES), axis=0)
                xhats[h, at, :] = xhat
                scaled[h, at, :] = ng * g * rs
            return carry

        lax.fori_loop(0, size // 32, step, 0)
        for copy in store(i):
            copy.start()
        at = pl.ds(pl.multiple_of(i * size, size), size)
        pairs = []
        for h in range(2):
            x = scaled[h, at, :]
            pairs += [(0, x), (1, x * xhats[h, at, :])]
        out = row_sums(pairs)
        for p in range(peers):
            sums[p, :, at] = out[0:2]
        return carry

    lax.fori_loop(0, rows // size, block, 0)
    for i in range(rows // size):
        for copy in store(i):
            copy.wait()


def taps_body(
    xhat_in, glu_in, sums, scaled, gain_sum, grad, small,
    rows_in, stack, columns, xhat, glu, sems,
):
    rows = grad.shape[1]
    size = 256
    loads = []
    for i in range(rows // size):
        at = pl.ds(i * size, size)
        loads.append(pltpu.make_async_copy(xhat_in.at[:, at], xhat.at[:, at], sems.at[i]))
        loads[i].start()
    load_glu = pltpu.make_async_copy(glu_in, glu, sems.at[rows // size])
    load_glu.start()
    peers = sums.shape[0]
    n = small.shape[0] - 1
    total = sums[0]
    for p in range(1, peers):
        total = total + sums[p]
    rows_in[...] = total * (1.0 / (2 * LANES * peers))
    spread(rows_in, stack, columns)
    for i in range(rows // size):
        loads[i].wait()

        def step(j, carry, i=i):
            at = pl.ds(pl.multiple_of(i * size + j * 64, 64), 64)
            for h in range(2):
                grad[h, at, :] = scaled[h, at, :] - columns[0, at] - xhat[h, at, :] * columns[1, at]
            return carry

        lax.fori_loop(0, size // 64, step, 0)
    load_glu.wait()
    for h in range(2):
        for lo, hi in ((0, 16), (16, n)):

            def tile(i, acc, h=h, lo=lo, hi=hi):
                acc = list(acc)
                for u in range(4):
                    r = pl.multiple_of(i * 32 + u * 8, 8)
                    c = grad[h, pl.ds(r, 8), :]
                    for k in range(lo, hi):
                        acc[k - lo] = acc[k - lo] + c * glu[h, pl.ds(r + PAD + 1 - n + k, 8), :]
                return tuple(acc)

            zero = tuple(jnp.zeros((8, LANES), F32) for _ in range(lo, hi))
            acc = lax.fori_loop(0, rows // 32, tile, zero)
            for k in range(lo, hi):
                small[k : k + 1, lanes(h)] = jnp.sum(acc[k - lo], axis=0, keepdims=True)
        small[n : n + 1, lanes(h)] = jnp.sum(gain_sum[h], axis=0, keepdims=True)


def pack_body(kept, received, small, other, out):
    outs = kept.shape[1]
    total = small[...] + other[...]
    low, high = total[0:16].astype(BF16), total[16:32].astype(BF16)
    for p in range(out.shape[0]):
        at = slice(p * 16, (p + 1) * 16)
        out[p, :, 0:outs] = (kept[at] + received[at]).astype(BF16)
        out[p, :, outs : outs + 256] = low
        out[p, :, outs + 256 : outs + 512] = high


def relay_body(got, out, held):
    outs = got.shape[2] - 512
    total = got[0].astype(F32)
    for p in range(1, got.shape[0]):
        total = total + got[p].astype(F32)
    held[...] = total[:, 0:outs]
    for p in range(out.shape[0]):
        out[p, :, 0:512] = total[0:8, outs:]
        out[p, :, 512:1024] = total[8:16, outs:]
        for i in range(2):
            for j in range(4):
                out[p, 4 * i + j : 4 * i + j + 1, 1024:1280] = held[
                    2 * p + i : 2 * p + i + 1, 256 * j : 256 * j + 256
                ]


def final_body(factor, got, proj, taps, gain):
    total = got[0]
    for p in range(1, got.shape[0]):
        total = total + got[p]
    total = total * factor
    taps[0:8] = total[:, 0:256]
    taps[16:24] = total[:, 256:512]
    taps[8:16] = total[:, 512:768]
    taps[24:31] = total[0:7, 768:1024]
    gain[...] = total[7:8, 768:1024]
    for i in range(2):
        for j in range(4):
            proj[i : i + 1, 256 * j : 256 * j + 256] = total[4 * i + j : 4 * i + j + 1, 1024:1280]


def moves(pairs, sems):
    copies = [pltpu.make_async_copy(x, y, sems.at[k]) for k, (x, y) in enumerate(pairs)]
    for copy in copies:
        copy.start()
    return copies


def glu_grad_rows(source, offset, taps, value, gate, out_value, out_gate, first, count):
    n = taps.shape[0]
    for h in range(2):
        weights = [jnp.broadcast_to(taps[k : k + 1, lanes(h)], (8, LANES)) for k in range(n)]

        def step(i, carry, h=h, weights=weights):
            tiles = []
            for u in range(4):
                r = offset + i * 32 + u * 8
                parts = [None, None]
                for k in range(n):
                    term = weights[k] * source[h, pl.ds(r + n - 1 - k, 8), :]
                    parts[k % 2] = term if parts[k % 2] is None else parts[k % 2] + term
                tiles.append(parts[0] + parts[1])
            at = pl.ds(pl.multiple_of(first + i * 32, 32), 32)
            sig = jax.nn.sigmoid(gate[at, lanes(h)].astype(F32))
            got = jnp.concatenate(tiles, axis=0) * sig
            out_value[at, lanes(h)] = got.astype(BF16)
            out_gate[at, lanes(h)] = (got * value[at, lanes(h)].astype(F32) * (1.0 - sig)).astype(BF16)
            return carry

        lax.fori_loop(0, count // 32, step, 0)


def glu_head_body(
    value_in, gate_in, grad, taps, value_grad, gate_grad, value, gate, out_value, out_gate, sems
):
    count = value.shape[0]
    at = pl.ds(0, count)
    for copy in moves(((value_in.at[at], value), (gate_in.at[at], gate)), sems):
        copy.wait()
    glu_grad_rows(grad, 0, taps, value, gate, out_value, out_gate, 0, count)
    for copy in moves(((out_value, value_grad.at[at]), (out_gate, gate_grad.at[at])), sems):
        copy.wait()


def glu_tail_body(
    value_in, gate_in, value_part, gate_part, grad, after, taps, value_grad, gate_grad,
    value, gate, out_value, out_gate, ext, sems,
):
    count = value.shape[0]
    rows = grad.shape[1]
    at = pl.ds(rows - count, count)
    loads = moves(((value_in.at[at], value), (gate_in.at[at], gate)), sems)
    for h in range(2):
        ext[h, 0:PAD, :] = grad[h, rows - PAD :, :]
        ext[h, PAD : 2 * PAD, :] = after[h]
    for load in loads:
        load.wait()
    glu_grad_rows(grad, rows - count, taps, value, gate, out_value, out_gate, 0, count - PAD)
    glu_grad_rows(ext, 0, taps, value, gate, out_value, out_gate, count - PAD, PAD)
    for copy in moves(((out_value, value_grad.at[at]), (out_gate, gate_grad.at[at])), sems):
        copy.wait()


def act_body(grad_in, weight_in, act, out_grad, weight, sems):
    rows = out_grad.shape[0]
    size = rows // 4
    load_weight = pltpu.make_async_copy(weight_in, weight, sems.at[4])
    load_weight.start()
    loads = []
    for c in range(4):
        at = pl.ds(c * size, size)
        loads.append(pltpu.make_async_copy(grad_in.at[at], out_grad.at[at], sems.at[c]))
        loads[c].start()
    load_weight.wait()
    for c in range(4):
        loads[c].wait()
        at = pl.ds(c * size, size)
        act[at] = lax.dot_general(out_grad[at], weight[...], NT, preferred_element_type=F32)


def proj_body(me, activ_in, grad_in, kept_out, sent_out, activ, out_grad, kept, sent, sems):
    chunks = 4
    outs = out_grad.shape[1]
    size = outs // chunks
    width = activ.shape[1]
    half = width // 2
    load_activ = pltpu.make_async_copy(activ_in, activ, sems.at[chunks])
    load_activ.start()
    loads = []
    for c in range(chunks):
        at = pl.ds(c * size, size)
        loads.append(pltpu.make_async_copy(grad_in.at[:, at], out_grad.at[:, at], sems.at[c]))
        loads[c].start()
    row = lax.broadcasted_iota(jnp.int32, (width, width), 0)
    col = lax.broadcasted_iota(jnp.int32, (width, width), 1)
    low = jnp.bitwise_and(row, half - 1)
    high = jnp.bitwise_xor(jnp.right_shift(row, 7), me[0])
    source = jnp.left_shift(jnp.right_shift(low, 1), 2) + 2 * high + jnp.bitwise_and(row, 1)
    order = (col == source).astype(F32).astype(BF16)
    load_activ.wait()
    placed = lax.dot_general(order, activ[...], NT, preferred_element_type=F32).astype(BF16)
    stores = []
    for c in range(chunks):
        loads[c].wait()
        at = pl.ds(c * size, size)
        got = jnp.dot(placed, out_grad[:, at], preferred_element_type=F32)
        kept[:, at] = got[:half]
        sent[:, at] = got[half:]
        stores.append(pltpu.make_async_copy(sent.at[:, at], sent_out.at[:, at], sems.at[c]))
        stores.append(pltpu.make_async_copy(kept.at[:, at], kept_out.at[:, at], sems.at[chunks + 1 + c]))
        stores[2 * c].start()
        stores[2 * c + 1].start()
    for store in stores:
        store.wait()


def over_tp(array):
    return lax.all_to_all(array, "tp", 0, 0, tiled=True)


def per_device(glu_value, glu_gate, conv_taps, channel_gain, proj_weight, out_grad):
    n = conv_taps.shape[0]
    rows, width = glu_value.shape
    peers = lax.axis_size("tp")
    outs = out_grad.shape[1]
    factor = 1.0 / math.sqrt(rows * lax.axis_size(SP))

    def wide(length):
        return ((2, length, LANES), F32, "near")

    def kept_wide(length):
        return ((2, length, LANES), F32, "far")

    stat = ((peers, 2, rows), F32, "any")
    dma = pltpu.SemaphoreType.DMA
    tall = ((rows, width), BF16)
    glu, edge, taps = kernel(
        glu_body,
        [wide(rows + PAD), wide(PAD), ((n, width), F32, "near")],
        (far(glu_value), far(glu_gate), far(conv_taps)),
        ins=[HBM] * 3,
        scratch=[tall, tall, dma((2, 5))],
    )
    edge = shifted(edge, 1)
    conv, stats, saved = kernel(
        conv_body,
        [wide(rows), ((8, rows), F32, "near"), kept_wide(rows + PAD)],
        (near(glu), near(taps)),
        out_specs=[VMEM, VMEM, HBM],
        scratch=[dma],
    )
    saved, _, conv, stats = kernel(
        head_body,
        [kept_wide(rows + PAD), wide(rows + PAD), wide(rows), stat],
        (far(saved), near(edge), near(glu), near(taps), near(conv), near(stats)),
        ins=[HBM],
        out_specs=[HBM, VMEM, VMEM, VMEM],
        aliases={0: 0, 2: 1, 4: 2},
        scratch=[((8, 256), F32), dma],
    )
    stats = over_tp(stats)
    (act_grad,) = kernel(
        act_body,
        [((rows, width), F32, "near")],
        (far(out_grad), far(proj_weight)),
        ins=[HBM] * 2,
        scratch=[((rows, outs), BF16), ((width, outs), BF16), dma((5,))],
    )
    stats, act_grad = lax.optimization_barrier((stats, act_grad))
    spreading = [((2, rows), F32), ((LANES, LANES), F32), ((2, rows, LANES), F32)]
    activ, xhat, scaled, sums, gain_sum = kernel(
        norm_body,
        [(*tall, "far"), kept_wide(rows), wide(rows), stat, wide(8)],
        (near(stats), near(conv), near(act_grad), channel_gain[None]),
        out_specs=[HBM] * 2 + [VMEM] * 3,
        scratch=[*spreading, tall, wide(rows)[:2], dma((2, 4))],
    )
    sums = over_tp(sums)
    share = ((width // 2, outs), F32)
    kept, sent = kernel(
        proj_body,
        [(*share, "far")] * 2,
        (lax.axis_index("core")[None], far(activ), far(out_grad)),
        ins=[SMEM, HBM, HBM],
        out_specs=[HBM] * 2,
        scratch=[tall, ((rows, outs), BF16), share, share, dma((9,))],
    )
    sums, sent, kept = lax.optimization_barrier((sums, sent, kept))
    received = swapped(sent)
    grad, small = kernel(
        taps_body,
        [wide(rows), ((n + 1, width), F32, "near")],
        (far(xhat), far(saved), near(sums), near(scaled), near(gain_sum)),
        ins=[HBM] * 2,
        scratch=[*spreading, wide(rows)[:2], wide(rows + PAD)[:2], dma((5,))],
    )
    other = swapped(small)
    (first,) = kernel(
        pack_body,
        [((8, 16, outs + 512), BF16, "any")],
        (near(kept), near(received), near(small), near(other)),
    )
    first = lax.all_to_all(first, "z", 0, 0, tiled=True)
    after = shifted(grad[:, :PAD], -1)
    gates = [((rows // 2, width), BF16)] * 4
    value_grad, gate_grad = kernel(
        glu_head_body,
        [(*tall, "far")] * 2,
        (far(glu_value), far(glu_gate), near(grad), conv_taps),
        ins=[HBM] * 2,
        out_specs=[HBM] * 2,
        scratch=[*gates, dma((2,))],
    )
    first, after, value_grad, gate_grad = lax.optimization_barrier((first, after, value_grad, gate_grad))
    (second,) = kernel(
        relay_body, [((8, 8, 1280), F32, "any")], (near(first),), scratch=[((16, outs), F32)]
    )
    second = lax.all_to_all(second, "y", 0, 0, tiled=True)
    value_grad, gate_grad = kernel(
        glu_tail_body,
        [(*tall, "far")] * 2,
        (
            far(glu_value), far(glu_gate), far(value_grad), far(gate_grad), near(grad),
            near(after), conv_taps,
        ),
        ins=[HBM] * 4,
        out_specs=[HBM] * 2,
        aliases={2: 0, 3: 1},
        scratch=[*gates, ((2, 2 * PAD, LANES), F32), dma((2,))],
    )
    second, value_grad, gate_grad = lax.optimization_barrier((second, value_grad, gate_grad))
    proj_grad, taps_grad, gain_grad = kernel(
        lambda *refs: final_body(factor, *refs),
        [((2, outs), F32, "any"), ((n, width), F32, "any"), ((1, width), F32, "any")],
        (near(second),),
    )
    return (value_grad, gate_grad, proj_grad, taps_grad, gain_grad.reshape(width))


def solution(mesh):
    finer = Mesh(mesh.devices.reshape(8, 8, 2, mesh.shape["tp"]), (*SP, "tp"))
    return jax.shard_map(
        per_device,
        mesh=finer,
        in_specs=(P(SP, "tp"), P(SP, "tp"), P(None, "tp"), P("tp"), P("tp", None), P(SP, None)),
        out_specs=(P(SP, "tp"), P(SP, "tp"), P(("tp", *SP), None), P(None, "tp"), P("tp")),
        check_vma=False,
    )
```

```python
import math

import jax
import jax.numpy as jnp
from jax import lax
from jax.experimental import pallas as pl
from jax.experimental.pallas import tpu as pltpu
from jax.sharding import Mesh
from jax.sharding import PartitionSpec as P


SP = ("z", "y", "core")
F32, BF16 = jnp.float32, jnp.bfloat16
LANES = 128
PAD = 32
NT = (((1,), (1,)), ((), ()))


def shifted(block, distance):
    devices = range(lax.axis_size(SP))
    route = [(i - distance, i) for i in devices if i - distance in devices]
    return lax.ppermute(block, SP, route)


def swapped(block):
    return lax.ppermute(block, "core", [(0, 1), (1, 0)])


def near(array):
    return pltpu.with_memory_space_constraint(array, pltpu.VMEM)


def far(array):
    return pltpu.with_memory_space_constraint(array, pltpu.HBM)


VMEM, HBM, SMEM = (pl.BlockSpec(memory_space=m) for m in (pltpu.VMEM, pltpu.HBM, pltpu.SMEM))


def kernel(body, outs, args, ins=(), out_specs=None, scratch=(), aliases=None, limit=16):
    shapes = {
        "near": pltpu.VMEM,
        "far": pltpu.HBM,
        "any": jax.ShapeDtypeStruct,
    }
    return pl.pallas_call(
        body,
        out_shape=[shapes[where](s, d) for s, d, where in outs],
        in_specs=list(ins) + [VMEM] * (len(args) - len(ins)),
        out_specs=out_specs or [VMEM] * len(outs),
        scratch_shapes=[pltpu.VMEM(*x) if isinstance(x, tuple) else x for x in scratch],
        input_output_aliases=aliases or {},
        compiler_params=pltpu.CompilerParams(vmem_limit_bytes=limit << 20),
    )(*args)


def lanes(h):
    return slice(h * LANES, (h + 1) * LANES)


def glu_body(value_in, gate_in, taps_in, glu, edge, taps, value, gate, sems):
    rows = value.shape[0]
    chunks = sems.shape[1] - 1
    size = rows // chunks
    load_taps = pltpu.make_async_copy(taps_in, taps, sems.at[0, chunks])
    loads = []
    for c in range(chunks):
        at = pl.ds(c * size, size)
        loads.append(pltpu.make_async_copy(value_in.at[at], value.at[at], sems.at[0, c]))
        loads.append(pltpu.make_async_copy(gate_in.at[at], gate.at[at], sems.at[1, c]))
    for load in loads:
        load.start()
    load_taps.start()
    for c in range(chunks):
        loads[2 * c].wait()
        loads[2 * c + 1].wait()

        def step(i, carry, c=c):
            r = pl.multiple_of(c * size + i * 64, 64)
            for h in range(2):
                v = value[pl.ds(r, 64), lanes(h)].astype(F32)
                g = gate[pl.ds(r, 64), lanes(h)].astype(F32)
                glu[h, pl.ds(PAD + r, 64), :] = v * jax.nn.sigmoid(g)
            return carry

        lax.fori_loop(0, size // 64, step, 0)
    for h in range(2):
        edge[h] = glu[h, rows : rows + PAD, :]
    load_taps.wait()


def conv_rows(glu, taps, conv, start, count):
    n = taps.shape[0]
    for h in range(2):
        weights = [jnp.broadcast_to(taps[k : k + 1, lanes(h)], (8, LANES)) for k in range(n)]

        def step(i, carry, h=h, weights=weights):
            for u in range(4):
                r = start + i * 32 + u * 8
                parts = [None, None]
                for k in range(n):
                    term = weights[k] * glu[h, pl.ds(r + PAD + 1 - n + k, 8), :]
                    parts[k % 2] = term if parts[k % 2] is None else parts[k % 2] + term
                conv[h, pl.ds(pl.multiple_of(r, 8), 8), :] = parts[0] + parts[1]
            return carry

        lax.fori_loop(0, count // 32, step, 0)


def split(x):
    high = x.astype(BF16)
    return high, (x - high.astype(F32)).astype(BF16)


def selector(row):
    sub = lax.broadcasted_iota(jnp.int32, (8, LANES), 0)
    return (sub == row).astype(F32).astype(BF16)


def row_sums(pairs):
    total = None
    for row, x in pairs:
        pick = selector(row)
        for part in split(x):
            term = lax.dot_general(pick, part, NT, preferred_element_type=F32)
            total = term if total is None else total + term
    return total


def conv_stats(conv, stats, start, count):
    def step(i, carry):
        r = pl.multiple_of(start + i * 256, 256)
        pairs = []
        for h in range(2):
            c = conv[h, pl.ds(r, 256), :]
            pairs += [(0, c), (1, c * c)]
        stats[:, pl.ds(r, 256)] = row_sums(pairs)
        return carry

    lax.fori_loop(0, count // 256, step, 0)


def conv_body(glu, taps, conv, stats, saved, sem):
    rows = conv.shape[1]
    store = pltpu.make_async_copy(
        glu.at[:, pl.ds(PAD, rows)], saved.at[:, pl.ds(PAD, rows)], sem
    )
    store.start()
    conv_rows(glu, taps, conv, 256, rows - 256)
    conv_stats(conv, stats, 256, rows - 256)
    store.wait()


def head_body(saved_in, edge, glu_in, taps, conv_in, stats_in, saved, glu, conv, sent, stats, sem):
    store = pltpu.make_async_copy(edge, saved.at[:, pl.ds(0, PAD)], sem)
    store.start()
    for h in range(2):
        glu[h, 0:PAD, :] = edge[h]
    conv_rows(glu, taps, conv, 0, 256)
    conv_stats(conv, stats, 0, 256)
    rows = conv.shape[1]
    for p in range(sent.shape[0]):
        sent[p, :, 0:256] = stats[0:2]
        sent[p, :, 256:rows] = stats_in[0:2, 256:rows]
    store.wait()


def spread(rows, stack, columns):
    stats, length = rows.shape
    blocks = length // LANES
    stack[...] = jnp.zeros(stack.shape, F32)
    for s in range(stats):
        for b in range(blocks):
            stack[s * blocks + b : s * blocks + b + 1, :] = rows[s : s + 1, b * LANES : (b + 1) * LANES]
    turned = stack[...].T
    for s in range(stats):
        for b in range(blocks):
            j = s * blocks + b
            columns[s, b * LANES : (b + 1) * LANES] = jnp.broadcast_to(
                turned[:, j : j + 1], (LANES, LANES)
            )


def norm_body(
    stats, conv, act_grad, gain, activ_out, xhat_out, scaled, sums, gain_sum,
    rows_in, stack, columns, activ, xhats, sems,
):
    peers = stats.shape[0]
    rows = conv.shape[1]
    channels = 2 * LANES * peers
    total = stats[0]
    for p in range(1, peers):
        total = total + stats[p]
    mean = total[0:1] * (1.0 / channels)
    rows_in[0:1, :] = lax.rsqrt(total[1:2] * (1.0 / channels) - mean * mean + 1e-05)
    rows_in[1:2, :] = mean
    spread(rows_in, stack, columns)
    for h in range(2):
        gain_sum[h] = jnp.zeros((8, LANES), F32)
    size = 256

    def store(i):
        at = pl.ds(pl.multiple_of(i * size, size), size)
        return (
            pltpu.make_async_copy(activ.at[at], activ_out.at[at], sems.at[0, i]),
            pltpu.make_async_copy(xhats.at[:, at], xhat_out.at[:, at], sems.at[1, i]),
        )

    def block(i, carry):
        def step(j, carry):
            at = pl.ds(pl.multiple_of(i * size + j * 32, 32), 32)
            rs, mu = columns[0, at], columns[1, at]
            for h in range(2):
                g = gain[0:1, lanes(h)]
                xhat = (conv[h, at, :] - mu) * rs
                normed = xhat * g
                sig = jax.nn.sigmoid(normed)
                act = normed * sig
                activ[at, lanes(h)] = act.astype(BF16)
                ng = act_grad[at, lanes(h)] * (sig + act * (1.0 - sig))
                gain_sum[h] += jnp.sum((ng * xhat).reshape(4, 8, LANES), axis=0)
                xhats[h, at, :] = xhat
                scaled[h, at, :] = ng * g * rs
            return carry

        lax.fori_loop(0, size // 32, step, 0)
        for copy in store(i):
            copy.start()
        at = pl.ds(pl.multiple_of(i * size, size), size)
        pairs = []
        for h in range(2):
            x = scaled[h, at, :]
            pairs += [(0, x), (1, x * xhats[h, at, :])]
        out = row_sums(pairs)
        for p in range(peers):
            sums[p, :, at] = out[0:2]
        return carry

    lax.fori_loop(0, rows // size, block, 0)
    for i in range(rows // size):
        for copy in store(i):
            copy.wait()


def taps_body(
    taps_count, xhat_in, glu_in, sent_in, sums, scaled, gain_sum, grad, sent,
    rows_in, stack, columns, xhat, glu, small, sems,
):
    rows = grad.shape[1]
    size = 256
    loads = []
    for i in range(rows // size):
        at = pl.ds(i * size, size)
        loads.append(pltpu.make_async_copy(xhat_in.at[:, at], xhat.at[:, at], sems.at[i]))
        loads[i].start()
    load_glu = pltpu.make_async_copy(glu_in, glu, sems.at[rows // size])
    load_glu.start()
    peers = sums.shape[0]
    n = taps_count
    total = sums[0]
    for p in range(1, peers):
        total = total + sums[p]
    rows_in[...] = total * (1.0 / (2 * LANES * peers))
    spread(rows_in, stack, columns)
    for i in range(rows // size):
        loads[i].wait()

        def step(j, carry, i=i):
            at = pl.ds(pl.multiple_of(i * size + j * 64, 64), 64)
            for h in range(2):
                grad[h, at, :] = scaled[h, at, :] - columns[0, at] - xhat[h, at, :] * columns[1, at]
            return carry

        lax.fori_loop(0, size // 64, step, 0)
    load_glu.wait()
    for h in range(2):
        for lo, hi in ((0, 16), (16, n)):

            def tile(i, acc, h=h, lo=lo, hi=hi):
                acc = list(acc)
                for u in range(4):
                    r = pl.multiple_of(i * 32 + u * 8, 8)
                    c = grad[h, pl.ds(r, 8), :]
                    for k in range(lo, hi):
                        acc[k - lo] = acc[k - lo] + c * glu[h, pl.ds(r + PAD + 1 - n + k, 8), :]
                return tuple(acc)

            zero = tuple(jnp.zeros((8, LANES), F32) for _ in range(lo, hi))
            acc = lax.fori_loop(0, rows // 32, tile, zero)
            for k in range(lo, hi):
                small[k : k + 1, lanes(h)] = jnp.sum(acc[k - lo], axis=0, keepdims=True)
        small[n : n + 1, lanes(h)] = jnp.sum(gain_sum[h], axis=0, keepdims=True)
    top = sent.shape[0] - 8
    for q in range(4):
        sent[top:, 256 * q : 256 * q + 256] = small[8 * q : 8 * q + 8]


def pack_body(kept, sent, received, out):
    rows, outs = kept.shape
    total = sent[rows:] + received[rows:]
    small = jnp.concatenate([total[:, 0:512], total[:, 512:1024]], axis=0).astype(BF16)
    for p in range(out.shape[0]):
        at = slice(p * 16, (p + 1) * 16)
        out[p, :, 0:outs] = (kept[at] + received[at]).astype(BF16)
        out[p, :, outs:] = small


def relay_body(got, out, held):
    outs = got.shape[2] - 512
    total = got[0].astype(F32)
    for p in range(1, got.shape[0]):
        total = total + got[p].astype(F32)
    held[...] = total[:, 0:outs]
    for p in range(out.shape[0]):
        out[p, :, 0:512] = total[0:8, outs:]
        out[p, :, 512:1024] = total[8:16, outs:]
        for i in range(2):
            for j in range(4):
                out[p, 4 * i + j : 4 * i + j + 1, 1024:1280] = held[
                    2 * p + i : 2 * p + i + 1, 256 * j : 256 * j + 256
                ]


def final_body(factor, got, proj, taps, gain):
    total = got[0]
    for p in range(1, got.shape[0]):
        total = total + got[p]
    total = total * factor
    taps[0:8] = total[:, 0:256]
    taps[8:16] = total[:, 256:512]
    taps[16:24] = total[:, 512:768]
    taps[24:31] = total[0:7, 768:1024]
    gain[...] = total[7:8, 768:1024]
    for i in range(2):
        for j in range(4):
            proj[i : i + 1, 256 * j : 256 * j + 256] = total[4 * i + j : 4 * i + j + 1, 1024:1280]


def moves(pairs, sems):
    copies = [pltpu.make_async_copy(x, y, sems.at[k]) for k, (x, y) in enumerate(pairs)]
    for copy in copies:
        copy.start()
    return copies


def glu_grad_rows(source, offset, taps, value, gate, out_value, out_gate, first, count):
    n = taps.shape[0]
    for h in range(2):
        weights = [jnp.broadcast_to(taps[k : k + 1, lanes(h)], (8, LANES)) for k in range(n)]

        def step(i, carry, h=h, weights=weights):
            tiles = []
            for u in range(4):
                r = offset + i * 32 + u * 8
                parts = [None, None]
                for k in range(n):
                    term = weights[k] * source[h, pl.ds(r + n - 1 - k, 8), :]
                    parts[k % 2] = term if parts[k % 2] is None else parts[k % 2] + term
                tiles.append(parts[0] + parts[1])
            at = pl.ds(pl.multiple_of(first + i * 32, 32), 32)
            sig = jax.nn.sigmoid(gate[at, lanes(h)].astype(F32))
            got = jnp.concatenate(tiles, axis=0) * sig
            out_value[at, lanes(h)] = got.astype(BF16)
            out_gate[at, lanes(h)] = (got * value[at, lanes(h)].astype(F32) * (1.0 - sig)).astype(BF16)
            return carry

        lax.fori_loop(0, count // 32, step, 0)


def glu_head_body(
    value_in, gate_in, grad, taps, value_grad, gate_grad, value, gate, out_value, out_gate, sems
):
    count = value.shape[0]
    at = pl.ds(0, count)
    for copy in moves(((value_in.at[at], value), (gate_in.at[at], gate)), sems):
        copy.wait()
    glu_grad_rows(grad, 0, taps, value, gate, out_value, out_gate, 0, count)
    for copy in moves(((out_value, value_grad.at[at]), (out_gate, gate_grad.at[at])), sems):
        copy.wait()


def glu_tail_body(
    value_in, gate_in, value_part, gate_part, grad, after, taps, value_grad, gate_grad,
    value, gate, out_value, out_gate, ext, sems,
):
    count = value.shape[0]
    rows = grad.shape[1]
    at = pl.ds(rows - count, count)
    loads = moves(((value_in.at[at], value), (gate_in.at[at], gate)), sems)
    for h in range(2):
        ext[h, 0:PAD, :] = grad[h, rows - PAD :, :]
        ext[h, PAD : 2 * PAD, :] = after[h]
    for load in loads:
        load.wait()
    glu_grad_rows(grad, rows - count, taps, value, gate, out_value, out_gate, 0, count - PAD)
    glu_grad_rows(ext, 0, taps, value, gate, out_value, out_gate, count - PAD, PAD)
    for copy in moves(((out_value, value_grad.at[at]), (out_gate, gate_grad.at[at])), sems):
        copy.wait()


def act_body(grad_in, weight_in, act, out_grad, weight, sems):
    rows = out_grad.shape[0]
    size = rows // 4
    load_weight = pltpu.make_async_copy(weight_in, weight, sems.at[4])
    load_weight.start()
    loads = []
    for c in range(4):
        at = pl.ds(c * size, size)
        loads.append(pltpu.make_async_copy(grad_in.at[at], out_grad.at[at], sems.at[c]))
        loads[c].start()
    load_weight.wait()
    for c in range(4):
        loads[c].wait()
        at = pl.ds(c * size, size)
        act[at] = lax.dot_general(out_grad[at], weight[...], NT, preferred_element_type=F32)


def proj_body(me, activ_in, grad_in, kept_out, sent, activ, out_grad, kept, sems):
    chunks = 4
    outs = out_grad.shape[1]
    size = outs // chunks
    width = activ.shape[1]
    half = width // 2
    load_activ = pltpu.make_async_copy(activ_in, activ, sems.at[chunks])
    load_activ.start()
    loads = []
    for c in range(chunks):
        at = pl.ds(c * size, size)
        loads.append(pltpu.make_async_copy(grad_in.at[:, at], out_grad.at[:, at], sems.at[c]))
        loads[c].start()
    row = lax.broadcasted_iota(jnp.int32, (width, width), 0)
    col = lax.broadcasted_iota(jnp.int32, (width, width), 1)
    low = jnp.bitwise_and(row, half - 1)
    high = jnp.bitwise_xor(jnp.right_shift(row, 7), me[0])
    source = jnp.left_shift(jnp.right_shift(low, 1), 2) + 2 * high + jnp.bitwise_and(row, 1)
    order = (col == source).astype(F32).astype(BF16)
    load_activ.wait()
    placed = lax.dot_general(order, activ[...], NT, preferred_element_type=F32).astype(BF16)
    stores = []
    for c in range(chunks):
        loads[c].wait()
        at = pl.ds(c * size, size)
        got = jnp.dot(placed, out_grad[:, at], preferred_element_type=F32)
        kept[:, at] = got[:half]
        sent[0:half, at] = got[half:]
        stores.append(pltpu.make_async_copy(kept.at[:, at], kept_out.at[:, at], sems.at[chunks + 1 + c]))
        stores[c].start()
    for store in stores:
        store.wait()


def over_tp(array):
    return lax.all_to_all(array, "tp", 0, 0, tiled=True)


def per_device(glu_value, glu_gate, conv_taps, channel_gain, proj_weight, out_grad):
    n = conv_taps.shape[0]
    rows, width = glu_value.shape
    peers = lax.axis_size("tp")
    outs = out_grad.shape[1]
    factor = 1.0 / math.sqrt(rows * lax.axis_size(SP))

    def wide(length):
        return ((2, length, LANES), F32, "near")

    def kept_wide(length):
        return ((2, length, LANES), F32, "far")

    stat = ((peers, 2, rows), F32, "any")
    dma = pltpu.SemaphoreType.DMA
    tall = ((rows, width), BF16)
    glu, edge, taps = kernel(
        glu_body,
        [wide(rows + PAD), wide(PAD), ((n, width), F32, "near")],
        (far(glu_value), far(glu_gate), far(conv_taps)),
        ins=[HBM] * 3,
        scratch=[tall, tall, dma((2, 5))],
    )
    edge = shifted(edge, 1)
    conv, stats, saved = kernel(
        conv_body,
        [wide(rows), ((8, rows), F32, "near"), kept_wide(rows + PAD)],
        (near(glu), near(taps)),
        out_specs=[VMEM, VMEM, HBM],
        scratch=[dma],
    )
    saved, _, conv, stats = kernel(
        head_body,
        [kept_wide(rows + PAD), wide(rows + PAD), wide(rows), stat],
        (far(saved), near(edge), near(glu), near(taps), near(conv), near(stats)),
        ins=[HBM],
        out_specs=[HBM, VMEM, VMEM, VMEM],
        aliases={0: 0, 2: 1, 4: 2},
        scratch=[((8, 256), F32), dma],
    )
    stats = over_tp(stats)
    (act_grad,) = kernel(
        act_body,
        [((rows, width), F32, "near")],
        (far(out_grad), far(proj_weight)),
        ins=[HBM] * 2,
        scratch=[((rows, outs), BF16), ((width, outs), BF16), dma((5,))],
    )
    stats, act_grad = lax.optimization_barrier((stats, act_grad))
    spreading = [((2, rows), F32), ((LANES, LANES), F32), ((2, rows, LANES), F32)]
    activ, xhat, scaled, sums, gain_sum = kernel(
        norm_body,
        [(*tall, "far"), kept_wide(rows), wide(rows), stat, wide(8)],
        (near(stats), near(conv), near(act_grad), channel_gain[None]),
        out_specs=[HBM] * 2 + [VMEM] * 3,
        scratch=[*spreading, tall, wide(rows)[:2], dma((2, 4))],
    )
    sums = over_tp(sums)
    share = ((width // 2, outs), F32)
    joint = ((width // 2 + 8, outs), F32, "near")
    kept, sent = kernel(
        proj_body,
        [(*share, "far"), joint],
        (lax.axis_index("core")[None], far(activ), far(out_grad)),
        ins=[SMEM, HBM, HBM],
        out_specs=[HBM, VMEM],
        scratch=[tall, ((rows, outs), BF16), share, dma((9,))],
    )
    sums, sent, kept = lax.optimization_barrier((sums, sent, kept))
    grad, sent = kernel(
        lambda *refs: taps_body(n, *refs),
        [wide(rows), joint],
        (far(xhat), far(saved), near(sent), near(sums), near(scaled), near(gain_sum)),
        ins=[HBM] * 2,
        aliases={2: 1},
        scratch=[*spreading, wide(rows)[:2], wide(rows + PAD)[:2], ((32, width), F32), dma((5,))],
    )
    received = swapped(sent)
    (first,) = kernel(
        pack_body, [((8, 16, outs + 512), BF16, "any")], (near(kept), near(sent), near(received))
    )
    first = lax.all_to_all(first, "z", 0, 0, tiled=True)
    after = shifted(grad[:, :PAD], -1)
    gates = [((rows // 2, width), BF16)] * 4
    value_grad, gate_grad = kernel(
        glu_head_body,
        [(*tall, "far")] * 2,
        (far(glu_value), far(glu_gate), near(grad), conv_taps),
        ins=[HBM] * 2,
        out_specs=[HBM] * 2,
        scratch=[*gates, dma((2,))],
    )
    first, after, value_grad, gate_grad = lax.optimization_barrier((first, after, value_grad, gate_grad))
    (second,) = kernel(
        relay_body, [((8, 8, 1280), F32, "any")], (near(first),), scratch=[((16, outs), F32)]
    )
    second = lax.all_to_all(second, "y", 0, 0, tiled=True)
    value_grad, gate_grad = kernel(
        glu_tail_body,
        [(*tall, "far")] * 2,
        (
            far(glu_value), far(glu_gate), far(value_grad), far(gate_grad), near(grad),
            near(after), conv_taps,
        ),
        ins=[HBM] * 4,
        out_specs=[HBM] * 2,
        aliases={2: 0, 3: 1},
        scratch=[*gates, ((2, 2 * PAD, LANES), F32), dma((2,))],
    )
    second, value_grad, gate_grad = lax.optimization_barrier((second, value_grad, gate_grad))
    proj_grad, taps_grad, gain_grad = kernel(
        lambda *refs: final_body(factor, *refs),
        [((2, outs), F32, "any"), ((n, width), F32, "any"), ((1, width), F32, "any")],
        (near(second),),
    )
    return (value_grad, gate_grad, proj_grad, taps_grad, gain_grad.reshape(width))


def solution(mesh):
    finer = Mesh(mesh.devices.reshape(8, 8, 2, mesh.shape["tp"]), (*SP, "tp"))
    return jax.shard_map(
        per_device,
        mesh=finer,
        in_specs=(P(SP, "tp"), P(SP, "tp"), P(None, "tp"), P("tp"), P("tp", None), P(SP, None)),
        out_specs=(P(SP, "tp"), P(SP, "tp"), P(("tp", *SP), None), P(None, "tp"), P("tp")),
        check_vma=False,
    )
```

```python
import math

import jax
import jax.numpy as jnp
from jax import lax
from jax.experimental import pallas as pl
from jax.experimental.pallas import tpu as pltpu
from jax.sharding import Mesh
from jax.sharding import PartitionSpec as P


SP = ("z", "y", "core")
F32, BF16 = jnp.float32, jnp.bfloat16
LANES = 128
PAD = 32
NT = (((1,), (1,)), ((), ()))


def shifted(block, distance):
    devices = range(lax.axis_size(SP))
    route = [(i - distance, i) for i in devices if i - distance in devices]
    return lax.ppermute(block, SP, route)


def swapped(block):
    return lax.ppermute(block, "core", [(0, 1), (1, 0)])


def near(array):
    return pltpu.with_memory_space_constraint(array, pltpu.VMEM)


def far(array):
    return pltpu.with_memory_space_constraint(array, pltpu.HBM)


VMEM, HBM, SMEM = (pl.BlockSpec(memory_space=m) for m in (pltpu.VMEM, pltpu.HBM, pltpu.SMEM))


def kernel(body, outs, args, ins=(), out_specs=None, scratch=(), aliases=None, limit=16):
    shapes = {
        "near": pltpu.VMEM,
        "far": pltpu.HBM,
        "any": jax.ShapeDtypeStruct,
    }
    return pl.pallas_call(
        body,
        out_shape=[shapes[where](s, d) for s, d, where in outs],
        in_specs=list(ins) + [VMEM] * (len(args) - len(ins)),
        out_specs=out_specs or [VMEM] * len(outs),
        scratch_shapes=[pltpu.VMEM(*x) if isinstance(x, tuple) else x for x in scratch],
        input_output_aliases=aliases or {},
        compiler_params=pltpu.CompilerParams(vmem_limit_bytes=limit << 20),
    )(*args)


def lanes(h):
    return slice(h * LANES, (h + 1) * LANES)


def glu_body(value_in, gate_in, taps_in, glu, edge, taps, value, gate, sems):
    rows = value.shape[0]
    chunks = sems.shape[1] - 1
    size = rows // chunks
    load_taps = pltpu.make_async_copy(taps_in, taps, sems.at[0, chunks])
    loads = []
    for c in range(chunks):
        at = pl.ds(c * size, size)
        loads.append(pltpu.make_async_copy(value_in.at[at], value.at[at], sems.at[0, c]))
        loads.append(pltpu.make_async_copy(gate_in.at[at], gate.at[at], sems.at[1, c]))
    for load in loads:
        load.start()
    load_taps.start()
    for c in range(chunks):
        loads[2 * c].wait()
        loads[2 * c + 1].wait()

        def step(i, carry, c=c):
            r = pl.multiple_of(c * size + i * 64, 64)
            for h in range(2):
                v = value[pl.ds(r, 64), lanes(h)].astype(F32)
                g = gate[pl.ds(r, 64), lanes(h)].astype(F32)
                glu[h, pl.ds(PAD + r, 64), :] = v * jax.nn.sigmoid(g)
            return carry

        lax.fori_loop(0, size // 64, step, 0)
    for h in range(2):
        edge[h] = glu[h, rows : rows + PAD, :]
    load_taps.wait()


def weighted(source, h, base, weights):
    parts = [[None, None] for _ in range(4)]
    for k, weight in enumerate(weights):
        for u in range(4):
            term = weight * source[h, pl.ds(base + k + u * 8, 8), :]
            old = parts[u][k % 2]
            parts[u][k % 2] = term if old is None else old + term
    return [p[0] + p[1] for p in parts]


def conv_rows(glu, taps, conv, start, count):
    n = taps.shape[0]
    for h in range(2):
        weights = [jnp.broadcast_to(taps[k : k + 1, lanes(h)], (8, LANES)) for k in range(n)]

        def step(i, carry, h=h, weights=weights):
            r = start + i * 32
            tiles = weighted(glu, h, r + PAD + 1 - n, weights)
            for u in range(4):
                conv[h, pl.ds(pl.multiple_of(r + u * 8, 8), 8), :] = tiles[u]
            return carry

        lax.fori_loop(0, count // 32, step, 0)


def split(x):
    high = x.astype(BF16)
    return high, (x - high.astype(F32)).astype(BF16)


def selector(row):
    sub = lax.broadcasted_iota(jnp.int32, (8, LANES), 0)
    return (sub == row).astype(F32).astype(BF16)


def row_sums(pairs):
    total = None
    for row, x in pairs:
        pick = selector(row)
        for part in split(x):
            term = lax.dot_general(pick, part, NT, preferred_element_type=F32)
            total = term if total is None else total + term
    return total


def conv_stats(conv, stats, start, count):
    def step(i, carry):
        r = pl.multiple_of(start + i * 256, 256)
        pairs = []
        for h in range(2):
            c = conv[h, pl.ds(r, 256), :]
            pairs += [(0, c), (1, c * c)]
        stats[:, pl.ds(r, 256)] = row_sums(pairs)
        return carry

    lax.fori_loop(0, count // 256, step, 0)


def conv_body(glu, taps, conv, stats):
    rows = conv.shape[1]
    conv_rows(glu, taps, conv, PAD, rows - PAD)
    conv_stats(conv, stats, 256, rows - 256)


def head_body(edge, glu_in, taps, conv_in, stats_in, glu, conv, sent, stats):
    for h in range(2):
        glu[h, 0:PAD, :] = edge[h]
    conv_rows(glu, taps, conv, 0, PAD)
    conv_stats(conv, stats, 0, 256)
    rows = conv.shape[1]
    for p in range(sent.shape[0]):
        sent[p, :, 0:256] = stats[0:2]
        sent[p, :, 256:rows] = stats_in[0:2, 256:rows]


def spread(rows, stack, columns):
    stats, length = rows.shape
    blocks = length // LANES
    stack[...] = jnp.zeros(stack.shape, F32)
    for s in range(stats):
        for b in range(blocks):
            stack[s * blocks + b : s * blocks + b + 1, :] = rows[s : s + 1, b * LANES : (b + 1) * LANES]
    turned = stack[...].T
    for s in range(stats):
        for b in range(blocks):
            j = s * blocks + b
            columns[s, b * LANES : (b + 1) * LANES] = jnp.broadcast_to(
                turned[:, j : j + 1], (LANES, LANES)
            )


def norm_body(
    stats, conv, act_grad, gain, activ, xhats, scaled, sums, gain_sum, rows_in, stack, columns
):
    peers = stats.shape[0]
    rows = conv.shape[1]
    channels = 2 * LANES * peers
    total = stats[0]
    for p in range(1, peers):
        total = total + stats[p]
    mean = total[0:1] * (1.0 / channels)
    rows_in[0:1, :] = lax.rsqrt(total[1:2] * (1.0 / channels) - mean * mean + 1e-05)
    rows_in[1:2, :] = mean
    spread(rows_in, stack, columns)
    for h in range(2):
        gain_sum[h] = jnp.zeros((8, LANES), F32)
    size = 256

    def block(i, carry):
        def step(j, carry):
            at = pl.ds(pl.multiple_of(i * size + j * 32, 32), 32)
            rs, mu = columns[0, at], columns[1, at]
            for h in range(2):
                g = gain[0:1, lanes(h)]
                xhat = (conv[h, at, :] - mu) * rs
                normed = xhat * g
                sig = jax.nn.sigmoid(normed)
                act = normed * sig
                activ[at, lanes(h)] = act.astype(BF16)
                ng = act_grad[at, lanes(h)] * (sig + act * (1.0 - sig))
                gain_sum[h] += jnp.sum((ng * xhat).reshape(4, 8, LANES), axis=0)
                xhats[h, at, :] = xhat
                scaled[h, at, :] = ng * g * rs
            return carry

        lax.fori_loop(0, size // 32, step, 0)
        at = pl.ds(pl.multiple_of(i * size, size), size)
        pairs = []
        for h in range(2):
            x = scaled[h, at, :]
            pairs += [(0, x), (1, x * xhats[h, at, :])]
        out = row_sums(pairs)
        for p in range(peers):
            sums[p, :, at] = out[0:2]
        return carry

    lax.fori_loop(0, rows // size, block, 0)


def taps_body(
    n, sent_in, sums, scaled, xhat, glu, gain_sum, grad, sent, rows_in, stack, columns, small
):
    rows = grad.shape[1]
    peers = sums.shape[0]
    total = sums[0]
    for p in range(1, peers):
        total = total + sums[p]
    rows_in[...] = total * (1.0 / (2 * LANES * peers))
    spread(rows_in, stack, columns)

    def step(j, carry):
        at = pl.ds(pl.multiple_of(j * 64, 64), 64)
        for h in range(2):
            grad[h, at, :] = scaled[h, at, :] - columns[0, at] - xhat[h, at, :] * columns[1, at]
        return carry

    lax.fori_loop(0, rows // 64, step, 0)
    for h in range(2):
        for lo, hi in ((0, 16), (16, n)):

            def tile(i, acc, h=h, lo=lo, hi=hi):
                acc = list(acc)
                r = pl.multiple_of(i * 32, 32)
                c = [grad[h, pl.ds(r + u * 8, 8), :] for u in range(4)]
                for u in range(4):
                    for k in range(lo, hi):
                        base = r + PAD + 1 - n + k
                        acc[k - lo] = acc[k - lo] + c[u] * glu[h, pl.ds(base + u * 8, 8), :]
                return tuple(acc)

            zero = tuple(jnp.zeros((8, LANES), F32) for _ in range(lo, hi))
            acc = lax.fori_loop(0, rows // 32, tile, zero)
            for k in range(lo, hi):
                small[k : k + 1, lanes(h)] = jnp.sum(acc[k - lo], axis=0, keepdims=True)
        small[n : n + 1, lanes(h)] = jnp.sum(gain_sum[h], axis=0, keepdims=True)
    top = sent.shape[0] - 8
    for q in range(4):
        sent[top:, 256 * q : 256 * q + 256] = small[8 * q : 8 * q + 8]


def pack_body(kept, sent, received, out):
    rows, outs = kept.shape
    total = sent[rows:] + received[rows:]
    small = jnp.concatenate([total[:, 0:512], total[:, 512:1024]], axis=0).astype(BF16)
    for p in range(out.shape[0]):
        at = slice(p * 16, (p + 1) * 16)
        out[p, :, 0:outs] = (kept[at] + received[at]).astype(BF16)
        out[p, :, outs:] = small


def relay_body(got, out, held):
    outs = got.shape[2] - 512
    total = got[0].astype(F32)
    for p in range(1, got.shape[0]):
        total = total + got[p].astype(F32)
    held[...] = total[:, 0:outs]
    for p in range(out.shape[0]):
        out[p, :, 0:512] = total[0:8, outs:]
        out[p, :, 512:1024] = total[8:16, outs:]
        for i in range(2):
            for j in range(4):
                out[p, 4 * i + j : 4 * i + j + 1, 1024:1280] = held[
                    2 * p + i : 2 * p + i + 1, 256 * j : 256 * j + 256
                ]


def final_body(factor, got, proj, taps, gain):
    total = got[0]
    for p in range(1, got.shape[0]):
        total = total + got[p]
    total = total * factor
    taps[0:8] = total[:, 0:256]
    taps[8:16] = total[:, 256:512]
    taps[16:24] = total[:, 512:768]
    taps[24:31] = total[0:7, 768:1024]
    gain[...] = total[7:8, 768:1024]
    for i in range(2):
        for j in range(4):
            proj[i : i + 1, 256 * j : 256 * j + 256] = total[4 * i + j : 4 * i + j + 1, 1024:1280]


def moves(pairs, sems):
    copies = [pltpu.make_async_copy(x, y, sems.at[k]) for k, (x, y) in enumerate(pairs)]
    for copy in copies:
        copy.start()
    return copies


def glu_grad_rows(source, offset, taps, value, gate, out_value, out_gate, first, count):
    n = taps.shape[0]
    for h in range(2):
        weights = [jnp.broadcast_to(taps[k : k + 1, lanes(h)], (8, LANES)) for k in range(n)]

        def step(i, carry, h=h, weights=weights):
            tiles = weighted(source, h, offset + i * 32, weights[::-1])
            at = pl.ds(pl.multiple_of(first + i * 32, 32), 32)
            sig = jax.nn.sigmoid(gate[at, lanes(h)].astype(F32))
            got = jnp.concatenate(tiles, axis=0) * sig
            out_value[at, lanes(h)] = got.astype(BF16)
            out_gate[at, lanes(h)] = (got * value[at, lanes(h)].astype(F32) * (1.0 - sig)).astype(BF16)
            return carry

        lax.fori_loop(0, count // 32, step, 0)


def glu_head_body(
    value_in, gate_in, grad, taps, value_grad, gate_grad, value, gate, out_value, out_gate, sems
):
    count = value.shape[0]
    at = pl.ds(0, count)
    for copy in moves(((value_in.at[at], value), (gate_in.at[at], gate)), sems):
        copy.wait()
    glu_grad_rows(grad, 0, taps, value, gate, out_value, out_gate, 0, count)
    for copy in moves(((out_value, value_grad.at[at]), (out_gate, gate_grad.at[at])), sems):
        copy.wait()


def glu_tail_body(
    value_in, gate_in, value_part, gate_part, grad, after, taps, value_grad, gate_grad,
    value, gate, out_value, out_gate, ext, sems,
):
    count = value.shape[0]
    rows = grad.shape[1]
    at = pl.ds(rows - count, count)
    loads = moves(((value_in.at[at], value), (gate_in.at[at], gate)), sems)
    for h in range(2):
        ext[h, 0:PAD, :] = grad[h, rows - PAD :, :]
        ext[h, PAD : 2 * PAD, :] = after[h]
    for load in loads:
        load.wait()
    if count > PAD:
        glu_grad_rows(grad, rows - count, taps, value, gate, out_value, out_gate, 0, count - PAD)
    glu_grad_rows(ext, 0, taps, value, gate, out_value, out_gate, count - PAD, PAD)
    for copy in moves(((out_value, value_grad.at[at]), (out_gate, gate_grad.at[at])), sems):
        copy.wait()


def act_body(out_grad, weight, act):
    act[...] = lax.dot_general(out_grad[...], weight[...], NT, preferred_element_type=F32)


def proj_body(me, activ, out_grad, kept, sent):
    width = activ.shape[1]
    half = width // 2
    row = lax.broadcasted_iota(jnp.int32, (width, width), 0)
    col = lax.broadcasted_iota(jnp.int32, (width, width), 1)
    low = jnp.bitwise_and(row, half - 1)
    high = jnp.bitwise_xor(jnp.right_shift(row, 7), me[0])
    source = jnp.left_shift(jnp.right_shift(low, 1), 2) + 2 * high + jnp.bitwise_and(row, 1)
    order = (col == source).astype(F32).astype(BF16)
    placed = lax.dot_general(order, activ[...], NT, preferred_element_type=F32).astype(BF16)
    kept[...] = jnp.dot(placed[:half], out_grad[...], preferred_element_type=F32)
    sent[0:half] = jnp.dot(placed[half:], out_grad[...], preferred_element_type=F32)


def over_tp(array):
    return lax.all_to_all(array, "tp", 0, 0, tiled=True)


def per_device(glu_value, glu_gate, conv_taps, channel_gain, proj_weight, out_grad):
    n = conv_taps.shape[0]
    rows, width = glu_value.shape
    peers = lax.axis_size("tp")
    outs = out_grad.shape[1]
    factor = 1.0 / math.sqrt(rows * lax.axis_size(SP))

    def wide(length):
        return ((2, length, LANES), F32, "near")

    stat = ((peers, 2, rows), F32, "near")
    dma = pltpu.SemaphoreType.DMA
    tall = ((rows, width), BF16)
    glu, edge, taps = kernel(
        glu_body,
        [wide(rows + PAD), wide(PAD), ((n, width), F32, "near")],
        (far(glu_value), far(glu_gate), far(conv_taps)),
        ins=[HBM] * 3,
        scratch=[tall, tall, dma((2, 5))],
    )
    edge = shifted(edge, 1)
    conv, stats = kernel(conv_body, [wide(rows), ((8, rows), F32, "near")], (near(glu), near(taps)))
    out_grad, stats = lax.optimization_barrier((near(out_grad), stats))
    (act_grad,) = kernel(
        act_body, [((rows, width), F32, "near")], (near(out_grad), near(proj_weight))
    )
    me = lax.axis_index("core")[None]
    edge, act_grad, me = lax.optimization_barrier((edge, act_grad, me))
    glu, conv, stats = kernel(
        head_body,
        [wide(rows + PAD), wide(rows), stat],
        (near(edge), near(glu), near(taps), near(conv), near(stats)),
        aliases={1: 0, 3: 1},
        scratch=[((8, 256), F32)],
    )
    stats = over_tp(stats)
    spreading = [((2, rows), F32), ((LANES, LANES), F32), ((2, rows, LANES), F32)]
    activ, xhat, scaled, sums, gain_sum = kernel(
        norm_body,
        [(*tall, "near"), wide(rows), wide(rows), stat, wide(8)],
        (near(stats), near(conv), near(act_grad), channel_gain[None]),
        scratch=spreading,
    )
    sums = over_tp(sums)
    sums, activ = lax.optimization_barrier((sums, activ))
    joint = ((width // 2 + 8, outs), F32, "near")
    kept, sent = kernel(
        proj_body,
        [((width // 2, outs), F32, "near"), joint],
        (me, near(activ), near(out_grad)),
        ins=[SMEM],
    )
    grad, sent = kernel(
        lambda *refs: taps_body(n, *refs),
        [wide(rows), joint],
        (near(sent), near(sums), near(scaled), near(xhat), near(glu), near(gain_sum)),
        aliases={0: 1},
        scratch=[*spreading, ((32, width), F32)],
    )
    received = swapped(sent)
    (first,) = kernel(
        pack_body, [((8, 16, outs + 512), BF16, "any")], (near(kept), near(sent), near(received))
    )
    first = lax.all_to_all(first, "z", 0, 0, tiled=True)
    after = shifted(grad[:, :PAD], -1)

    def gates(length):
        return [((length, width), BF16)] * 4

    value_grad, gate_grad = kernel(
        glu_head_body,
        [(*tall, "far")] * 2,
        (far(glu_value), far(glu_gate), near(grad), conv_taps),
        ins=[HBM] * 2,
        out_specs=[HBM] * 2,
        scratch=[*gates(rows - PAD), dma((2,))],
    )
    after, value_grad, gate_grad = lax.optimization_barrier((after, value_grad, gate_grad))
    value_grad, gate_grad = kernel(
        glu_tail_body,
        [(*tall, "far")] * 2,
        (
            far(glu_value), far(glu_gate), far(value_grad), far(gate_grad), near(grad),
            near(after), conv_taps,
        ),
        ins=[HBM] * 4,
        out_specs=[HBM] * 2,
        aliases={2: 0, 3: 1},
        scratch=[*gates(PAD), ((2, 2 * PAD, LANES), F32), dma((2,))],
    )
    first, value_grad, gate_grad = lax.optimization_barrier((first, value_grad, gate_grad))
    (second,) = kernel(
        relay_body, [((8, 8, 1280), F32, "near")], (near(first),), scratch=[((16, outs), F32)]
    )
    second = lax.all_to_all(second, "y", 0, 0, tiled=True)
    proj_grad, taps_grad, gain_grad = kernel(
        lambda *refs: final_body(factor, *refs),
        [((2, outs), F32, "any"), ((n, width), F32, "any"), ((1, width), F32, "any")],
        (near(second),),
    )
    return (value_grad, gate_grad, proj_grad, taps_grad, gain_grad.reshape(width))


def solution(mesh):
    finer = Mesh(mesh.devices.reshape(8, 8, 2, mesh.shape["tp"]), (*SP, "tp"))
    return jax.shard_map(
        per_device,
        mesh=finer,
        in_specs=(P(SP, "tp"), P(SP, "tp"), P(None, "tp"), P("tp"), P("tp", None), P(SP, None)),
        out_specs=(P(SP, "tp"), P(SP, "tp"), P(("tp", *SP), None), P(None, "tp"), P("tp")),
        check_vma=False,
    )
```

```python
import math

import jax
import jax.numpy as jnp
from jax import lax
from jax.experimental import pallas as pl
from jax.experimental.pallas import tpu as pltpu
from jax.sharding import Mesh
from jax.sharding import PartitionSpec as P


SP = ("z", "y", "core")
F32, BF16 = jnp.float32, jnp.bfloat16
LANES = 128
PAD = 32
NT = (((1,), (1,)), ((), ()))


def shifted(block, distance):
    devices = range(lax.axis_size(SP))
    route = [(i - distance, i) for i in devices if i - distance in devices]
    return lax.ppermute(block, SP, route)


def swapped(block):
    return lax.ppermute(block, "core", [(0, 1), (1, 0)])


def near(array):
    return pltpu.with_memory_space_constraint(array, pltpu.VMEM)


def far(array):
    return pltpu.with_memory_space_constraint(array, pltpu.HBM)


VMEM, HBM, SMEM = (pl.BlockSpec(memory_space=m) for m in (pltpu.VMEM, pltpu.HBM, pltpu.SMEM))


def kernel(body, outs, args, ins=(), out_specs=None, scratch=(), aliases=None, limit=16):
    shapes = {
        "near": pltpu.VMEM,
        "far": pltpu.HBM,
        "any": jax.ShapeDtypeStruct,
    }
    return pl.pallas_call(
        body,
        out_shape=[shapes[where](s, d) for s, d, where in outs],
        in_specs=list(ins) + [VMEM] * (len(args) - len(ins)),
        out_specs=out_specs or [VMEM] * len(outs),
        scratch_shapes=[pltpu.VMEM(*x) if isinstance(x, tuple) else x for x in scratch],
        input_output_aliases=aliases or {},
        compiler_params=pltpu.CompilerParams(vmem_limit_bytes=limit << 20),
    )(*args)


def lanes(h):
    return slice(h * LANES, (h + 1) * LANES)


def glu_body(value_in, gate_in, taps_in, glu, edge, taps, value, gate, sems):
    rows = value.shape[0]
    chunks = sems.shape[1] - 1
    size = rows // chunks
    load_taps = pltpu.make_async_copy(taps_in, taps, sems.at[0, chunks])
    loads = []
    for c in range(chunks):
        at = pl.ds(c * size, size)
        loads.append(pltpu.make_async_copy(value_in.at[at], value.at[at], sems.at[0, c]))
        loads.append(pltpu.make_async_copy(gate_in.at[at], gate.at[at], sems.at[1, c]))
    for load in loads:
        load.start()
    load_taps.start()
    for c in range(chunks):
        loads[2 * c].wait()
        loads[2 * c + 1].wait()

        def step(i, carry, c=c):
            r = pl.multiple_of(c * size + i * 64, 64)
            for h in range(2):
                v = value[pl.ds(r, 64), lanes(h)].astype(F32)
                g = gate[pl.ds(r, 64), lanes(h)].astype(F32)
                glu[h, pl.ds(PAD + r, 64), :] = v * jax.nn.sigmoid(g)
            return carry

        lax.fori_loop(0, size // 64, step, 0)
    for h in range(2):
        edge[h] = glu[h, rows : rows + PAD, :]
    load_taps.wait()


def weighted(source, h, base, weights):
    parts = [[None, None] for _ in range(4)]
    for k, weight in enumerate(weights):
        for u in range(4):
            term = weight * source[h, pl.ds(base + k + u * 8, 8), :]
            old = parts[u][k % 2]
            parts[u][k % 2] = term if old is None else old + term
    return [p[0] + p[1] for p in parts]


def conv_rows(glu, taps, conv, start, count):
    n = taps.shape[0]
    for h in range(2):
        weights = [jnp.broadcast_to(taps[k : k + 1, lanes(h)], (8, LANES)) for k in range(n)]

        def step(i, carry, h=h, weights=weights):
            r = start + i * 32
            tiles = weighted(glu, h, r + PAD + 1 - n, weights)
            for u in range(4):
                conv[h, pl.ds(pl.multiple_of(r + u * 8, 8), 8), :] = tiles[u]
            return carry

        lax.fori_loop(0, count // 32, step, 0)


def split(x):
    high = x.astype(BF16)
    return high, (x - high.astype(F32)).astype(BF16)


def selector(row):
    sub = lax.broadcasted_iota(jnp.int32, (8, LANES), 0)
    return (sub == row).astype(F32).astype(BF16)


def row_sums(pairs):
    total = None
    for row, x in pairs:
        pick = selector(row)
        for part in split(x):
            term = lax.dot_general(pick, part, NT, preferred_element_type=F32)
            total = term if total is None else total + term
    return total


def conv_stats(conv, stats, start, count):
    def step(i, carry):
        r = pl.multiple_of(start + i * 256, 256)
        pairs = []
        for h in range(2):
            c = conv[h, pl.ds(r, 256), :]
            pairs += [(0, c), (1, c * c)]
        stats[:, pl.ds(r, 256)] = row_sums(pairs)
        return carry

    lax.fori_loop(0, count // 256, step, 0)


def conv_body(grad_in, weight_in, glu, taps, conv, stats, out_grad, weight, sems):
    rows = conv.shape[1]
    loads = moves(((weight_in, weight), (grad_in, out_grad)), sems)
    conv_rows(glu, taps, conv, PAD, rows - PAD)
    conv_stats(conv, stats, 256, rows - 256)
    for load in loads:
        load.wait()


def head_body(edge, glu_in, taps, conv_in, stats_in, glu, conv, sent, stats):
    for h in range(2):
        glu[h, 0:PAD, :] = edge[h]
    conv_rows(glu, taps, conv, 0, PAD)
    conv_stats(conv, stats, 0, 256)
    rows = conv.shape[1]
    for p in range(sent.shape[0]):
        sent[p, :, 0:256] = stats[0:2]
        sent[p, :, 256:rows] = stats_in[0:2, 256:rows]


def spread(rows, stack, columns):
    stats, length = rows.shape
    blocks = length // LANES
    stack[...] = jnp.zeros(stack.shape, F32)
    for s in range(stats):
        for b in range(blocks):
            stack[s * blocks + b : s * blocks + b + 1, :] = rows[s : s + 1, b * LANES : (b + 1) * LANES]
    turned = stack[...].T
    for s in range(stats):
        for b in range(blocks):
            j = s * blocks + b
            columns[s, b * LANES : (b + 1) * LANES] = jnp.broadcast_to(
                turned[:, j : j + 1], (LANES, LANES)
            )


def norm_body(
    stats, conv, act_grad, gain, activ, xhats, scaled, sums, gain_sum, rows_in, stack, columns
):
    peers = stats.shape[0]
    rows = conv.shape[1]
    channels = 2 * LANES * peers
    total = stats[0]
    for p in range(1, peers):
        total = total + stats[p]
    mean = total[0:1] * (1.0 / channels)
    rows_in[0:1, :] = lax.rsqrt(total[1:2] * (1.0 / channels) - mean * mean + 1e-05)
    rows_in[1:2, :] = mean
    spread(rows_in, stack, columns)
    for h in range(2):
        gain_sum[h] = jnp.zeros((8, LANES), F32)
    size = 256

    def block(i, carry):
        def step(j, carry):
            at = pl.ds(pl.multiple_of(i * size + j * 32, 32), 32)
            rs, mu = columns[0, at], columns[1, at]
            for h in range(2):
                g = gain[0:1, lanes(h)]
                xhat = (conv[h, at, :] - mu) * rs
                normed = xhat * g
                sig = jax.nn.sigmoid(normed)
                act = normed * sig
                activ[at, lanes(h)] = act.astype(BF16)
                ng = act_grad[at, lanes(h)] * (sig + act * (1.0 - sig))
                gain_sum[h] += jnp.sum((ng * xhat).reshape(4, 8, LANES), axis=0)
                xhats[h, at, :] = xhat
                scaled[h, at, :] = ng * g * rs
            return carry

        lax.fori_loop(0, size // 32, step, 0)
        at = pl.ds(pl.multiple_of(i * size, size), size)
        pairs = []
        for h in range(2):
            x = scaled[h, at, :]
            pairs += [(0, x), (1, x * xhats[h, at, :])]
        out = row_sums(pairs)
        for p in range(peers):
            sums[p, :, at] = out[0:2]
        return carry

    lax.fori_loop(0, rows // size, block, 0)


def taps_body(
    n, sent_in, sums, scaled, xhat, glu, gain_sum, grad, sent, rows_in, stack, columns, small
):
    rows = grad.shape[1]
    peers = sums.shape[0]
    total = sums[0]
    for p in range(1, peers):
        total = total + sums[p]
    rows_in[...] = total * (1.0 / (2 * LANES * peers))
    spread(rows_in, stack, columns)

    def step(j, carry):
        at = pl.ds(pl.multiple_of(j * 64, 64), 64)
        for h in range(2):
            grad[h, at, :] = scaled[h, at, :] - columns[0, at] - xhat[h, at, :] * columns[1, at]
        return carry

    lax.fori_loop(0, rows // 64, step, 0)
    for h in range(2):
        for lo, hi in ((0, 16), (16, n)):

            def tile(i, acc, h=h, lo=lo, hi=hi):
                acc = list(acc)
                r = pl.multiple_of(i * 32, 32)
                c = [grad[h, pl.ds(r + u * 8, 8), :] for u in range(4)]
                for u in range(4):
                    for k in range(lo, hi):
                        base = r + PAD + 1 - n + k
                        acc[k - lo] = acc[k - lo] + c[u] * glu[h, pl.ds(base + u * 8, 8), :]
                return tuple(acc)

            zero = tuple(jnp.zeros((8, LANES), F32) for _ in range(lo, hi))
            acc = lax.fori_loop(0, rows // 32, tile, zero)
            for k in range(lo, hi):
                small[k : k + 1, lanes(h)] = jnp.sum(acc[k - lo], axis=0, keepdims=True)
        small[n : n + 1, lanes(h)] = jnp.sum(gain_sum[h], axis=0, keepdims=True)
    top = sent.shape[0] - 8
    for q in range(4):
        sent[top:, 256 * q : 256 * q + 256] = small[8 * q : 8 * q + 8]


def pack_body(kept, sent, received, out):
    rows, outs = kept.shape
    total = sent[rows:] + received[rows:]
    small = jnp.concatenate([total[:, 0:512], total[:, 512:1024]], axis=0).astype(BF16)
    for p in range(out.shape[0]):
        at = slice(p * 16, (p + 1) * 16)
        out[p, :, 0:outs] = (kept[at] + received[at]).astype(BF16)
        out[p, :, outs:] = small


def relay_body(got, out, held):
    outs = got.shape[2] - 512
    total = got[0].astype(F32)
    for p in range(1, got.shape[0]):
        total = total + got[p].astype(F32)
    held[...] = total[:, 0:outs]
    for p in range(out.shape[0]):
        out[p, :, 0:512] = total[0:8, outs:]
        out[p, :, 512:1024] = total[8:16, outs:]
        for i in range(2):
            for j in range(4):
                out[p, 4 * i + j : 4 * i + j + 1, 1024:1280] = held[
                    2 * p + i : 2 * p + i + 1, 256 * j : 256 * j + 256
                ]


def final_body(factor, got, proj, taps, gain):
    total = got[0]
    for p in range(1, got.shape[0]):
        total = total + got[p]
    total = total * factor
    taps[0:8] = total[:, 0:256]
    taps[8:16] = total[:, 256:512]
    taps[16:24] = total[:, 512:768]
    taps[24:31] = total[0:7, 768:1024]
    gain[...] = total[7:8, 768:1024]
    for i in range(2):
        for j in range(4):
            proj[i : i + 1, 256 * j : 256 * j + 256] = total[4 * i + j : 4 * i + j + 1, 1024:1280]


def moves(pairs, sems):
    copies = [pltpu.make_async_copy(x, y, sems.at[k]) for k, (x, y) in enumerate(pairs)]
    for copy in copies:
        copy.start()
    return copies


def glu_grad_rows(source, offset, taps, value, gate, out_value, out_gate, first, count):
    n = taps.shape[0]
    for h in range(2):
        weights = [jnp.broadcast_to(taps[k : k + 1, lanes(h)], (8, LANES)) for k in range(n)]

        def step(i, carry, h=h, weights=weights):
            tiles = weighted(source, h, offset + i * 32, weights[::-1])
            at = pl.ds(pl.multiple_of(first + i * 32, 32), 32)
            sig = jax.nn.sigmoid(gate[at, lanes(h)].astype(F32))
            got = jnp.concatenate(tiles, axis=0) * sig
            out_value[at, lanes(h)] = got.astype(BF16)
            out_gate[at, lanes(h)] = (got * value[at, lanes(h)].astype(F32) * (1.0 - sig)).astype(BF16)
            return carry

        lax.fori_loop(0, count // 32, step, 0)


def glu_head_body(
    value_in, gate_in, grad, taps, value_grad, gate_grad, value, gate, out_value, out_gate, sems
):
    count = value.shape[0]
    at = pl.ds(0, count)
    for copy in moves(((value_in.at[at], value), (gate_in.at[at], gate)), sems):
        copy.wait()
    glu_grad_rows(grad, 0, taps, value, gate, out_value, out_gate, 0, count)
    for copy in moves(((out_value, value_grad.at[at]), (out_gate, gate_grad.at[at])), sems):
        copy.wait()


def glu_tail_body(
    value_in, gate_in, value_part, gate_part, grad, after, taps, value_grad, gate_grad,
    value, gate, out_value, out_gate, ext, sems,
):
    count = value.shape[0]
    rows = grad.shape[1]
    at = pl.ds(rows - count, count)
    loads = moves(((value_in.at[at], value), (gate_in.at[at], gate)), sems)
    for h in range(2):
        ext[h, 0:PAD, :] = grad[h, rows - PAD :, :]
        ext[h, PAD : 2 * PAD, :] = after[h]
    for load in loads:
        load.wait()
    if count > PAD:
        glu_grad_rows(grad, rows - count, taps, value, gate, out_value, out_gate, 0, count - PAD)
    glu_grad_rows(ext, 0, taps, value, gate, out_value, out_gate, count - PAD, PAD)
    for copy in moves(((out_value, value_grad.at[at]), (out_gate, gate_grad.at[at])), sems):
        copy.wait()


def act_body(out_grad, weight, act):
    act[...] = lax.dot_general(out_grad[...], weight[...], NT, preferred_element_type=F32)


def proj_body(me, activ, out_grad, kept, sent):
    width = activ.shape[1]
    half = width // 2
    row = lax.broadcasted_iota(jnp.int32, (width, width), 0)
    col = lax.broadcasted_iota(jnp.int32, (width, width), 1)
    low = jnp.bitwise_and(row, half - 1)
    high = jnp.bitwise_xor(jnp.right_shift(row, 7), me[0])
    source = jnp.left_shift(jnp.right_shift(low, 1), 2) + 2 * high + jnp.bitwise_and(row, 1)
    order = (col == source).astype(F32).astype(BF16)
    placed = lax.dot_general(order, activ[...], NT, preferred_element_type=F32).astype(BF16)
    kept[...] = jnp.dot(placed[:half], out_grad[...], preferred_element_type=F32)
    sent[0:half] = jnp.dot(placed[half:], out_grad[...], preferred_element_type=F32)


def over_tp(array):
    return lax.all_to_all(array, "tp", 0, 0, tiled=True)


def per_device(glu_value, glu_gate, conv_taps, channel_gain, proj_weight, out_grad):
    n = conv_taps.shape[0]
    rows, width = glu_value.shape
    peers = lax.axis_size("tp")
    outs = out_grad.shape[1]
    factor = 1.0 / math.sqrt(rows * lax.axis_size(SP))

    def wide(length):
        return ((2, length, LANES), F32, "near")

    stat = ((peers, 2, rows), F32, "near")
    dma = pltpu.SemaphoreType.DMA
    tall = ((rows, width), BF16)
    glu, edge, taps = kernel(
        glu_body,
        [wide(rows + PAD), wide(PAD), ((n, width), F32, "near")],
        (far(glu_value), far(glu_gate), far(conv_taps)),
        ins=[HBM] * 3,
        scratch=[tall, tall, dma((2, 5))],
    )
    edge = shifted(edge, 1)
    conv, stats, out_grad, weight = kernel(
        conv_body,
        [
            wide(rows),
            ((8, rows), F32, "near"),
            (out_grad.shape, BF16, "near"),
            (proj_weight.shape, BF16, "near"),
        ],
        (far(out_grad), far(proj_weight), near(glu), near(taps)),
        ins=[HBM] * 2,
        scratch=[dma((2,))],
    )
    (act_grad,) = kernel(act_body, [((rows, width), F32, "near")], (near(out_grad), near(weight)))
    me = lax.axis_index("core")[None]
    edge, act_grad, me = lax.optimization_barrier((edge, act_grad, me))
    glu, conv, stats = kernel(
        head_body,
        [wide(rows + PAD), wide(rows), stat],
        (near(edge), near(glu), near(taps), near(conv), near(stats)),
        aliases={1: 0, 3: 1},
        scratch=[((8, 256), F32)],
    )
    stats = over_tp(stats)
    spreading = [((2, rows), F32), ((LANES, LANES), F32), ((2, rows, LANES), F32)]
    activ, xhat, scaled, sums, gain_sum = kernel(
        norm_body,
        [(*tall, "near"), wide(rows), wide(rows), stat, wide(8)],
        (near(stats), near(conv), near(act_grad), channel_gain[None]),
        scratch=spreading,
    )
    sums = over_tp(sums)
    sums, activ = lax.optimization_barrier((sums, activ))
    joint = ((width // 2 + 8, outs), F32, "near")
    kept, sent = kernel(
        proj_body,
        [((width // 2, outs), F32, "near"), joint],
        (me, near(activ), near(out_grad)),
        ins=[SMEM],
    )
    grad, sent = kernel(
        lambda *refs: taps_body(n, *refs),
        [wide(rows), joint],
        (near(sent), near(sums), near(scaled), near(xhat), near(glu), near(gain_sum)),
        aliases={0: 1},
        scratch=[*spreading, ((32, width), F32)],
    )
    received = swapped(sent)
    (first,) = kernel(
        pack_body, [((8, 16, outs + 512), BF16, "any")], (near(kept), near(sent), near(received))
    )
    first = lax.all_to_all(first, "z", 0, 0, tiled=True)
    after = shifted(grad[:, :PAD], -1)

    def gates(length):
        return [((length, width), BF16)] * 4

    value_grad, gate_grad = kernel(
        glu_head_body,
        [(*tall, "far")] * 2,
        (far(glu_value), far(glu_gate), near(grad), conv_taps),
        ins=[HBM] * 2,
        out_specs=[HBM] * 2,
        scratch=[*gates(rows // 2), dma((2,))],
    )
    first, after, value_grad, gate_grad = lax.optimization_barrier((first, after, value_grad, gate_grad))
    (second,) = kernel(
        relay_body, [((8, 8, 1280), F32, "any")], (near(first),), scratch=[((16, outs), F32)]
    )
    second = lax.all_to_all(second, "y", 0, 0, tiled=True)
    value_grad, gate_grad = kernel(
        glu_tail_body,
        [(*tall, "far")] * 2,
        (
            far(glu_value), far(glu_gate), far(value_grad), far(gate_grad), near(grad),
            near(after), conv_taps,
        ),
        ins=[HBM] * 4,
        out_specs=[HBM] * 2,
        aliases={2: 0, 3: 1},
        scratch=[*gates(rows // 2), ((2, 2 * PAD, LANES), F32), dma((2,))],
    )
    second, value_grad, gate_grad = lax.optimization_barrier((second, value_grad, gate_grad))
    proj_grad, taps_grad, gain_grad = kernel(
        lambda *refs: final_body(factor, *refs),
        [((2, outs), F32, "any"), ((n, width), F32, "any"), ((1, width), F32, "any")],
        (near(second),),
    )
    return (value_grad, gate_grad, proj_grad, taps_grad, gain_grad.reshape(width))


def solution(mesh):
    finer = Mesh(mesh.devices.reshape(8, 8, 2, mesh.shape["tp"]), (*SP, "tp"))
    return jax.shard_map(
        per_device,
        mesh=finer,
        in_specs=(P(SP, "tp"), P(SP, "tp"), P(None, "tp"), P("tp"), P("tp", None), P(SP, None)),
        out_specs=(P(SP, "tp"), P(SP, "tp"), P(("tp", *SP), None), P(None, "tp"), P("tp")),
        check_vma=False,
    )
```

```python
import math

import jax
import jax.numpy as jnp
from jax import lax
from jax.experimental import pallas as pl
from jax.experimental.pallas import tpu as pltpu
from jax.sharding import Mesh
from jax.sharding import PartitionSpec as P


SP = ("z", "y", "core")
F32, BF16 = jnp.float32, jnp.bfloat16
LANES = 128
PAD = 32
NT = (((1,), (1,)), ((), ()))


def shifted(block, distance):
    devices = range(lax.axis_size(SP))
    route = [(i - distance, i) for i in devices if i - distance in devices]
    return lax.ppermute(block, SP, route)


def swapped(block):
    return lax.ppermute(block, "core", [(0, 1), (1, 0)])


def near(array):
    return pltpu.with_memory_space_constraint(array, pltpu.VMEM)


def far(array):
    return pltpu.with_memory_space_constraint(array, pltpu.HBM)


VMEM, HBM, SMEM = (pl.BlockSpec(memory_space=m) for m in (pltpu.VMEM, pltpu.HBM, pltpu.SMEM))


def kernel(body, outs, args, ins=(), out_specs=None, scratch=(), aliases=None, limit=16):
    shapes = {
        "near": pltpu.VMEM,
        "far": pltpu.HBM,
        "any": jax.ShapeDtypeStruct,
    }
    return pl.pallas_call(
        body,
        out_shape=[shapes[where](s, d) for s, d, where in outs],
        in_specs=list(ins) + [VMEM] * (len(args) - len(ins)),
        out_specs=out_specs or [VMEM] * len(outs),
        scratch_shapes=[pltpu.VMEM(*x) if isinstance(x, tuple) else x for x in scratch],
        input_output_aliases=aliases or {},
        compiler_params=pltpu.CompilerParams(vmem_limit_bytes=limit << 20),
    )(*args)


def lanes(h):
    return slice(h * LANES, (h + 1) * LANES)


def glu_body(value_in, gate_in, taps_in, glu, edge, taps, value, gate, sems):
    rows = value.shape[0]
    chunks = sems.shape[1] - 1
    size = rows // chunks
    load_taps = pltpu.make_async_copy(taps_in, taps, sems.at[0, chunks])
    loads = []
    for c in range(chunks):
        at = pl.ds(c * size, size)
        loads.append(pltpu.make_async_copy(value_in.at[at], value.at[at], sems.at[0, c]))
        loads.append(pltpu.make_async_copy(gate_in.at[at], gate.at[at], sems.at[1, c]))
    for load in loads:
        load.start()
    load_taps.start()
    for c in range(chunks):
        loads[2 * c].wait()
        loads[2 * c + 1].wait()

        def step(i, carry, c=c):
            r = pl.multiple_of(c * size + i * 64, 64)
            for h in range(2):
                v = value[pl.ds(r, 64), lanes(h)].astype(F32)
                g = gate[pl.ds(r, 64), lanes(h)].astype(F32)
                glu[h, pl.ds(PAD + r, 64), :] = v * jax.nn.sigmoid(g)
            return carry

        lax.fori_loop(0, size // 64, step, 0)
    for h in range(2):
        edge[h] = glu[h, rows : rows + PAD, :]
    load_taps.wait()


def weighted(source, h, base, weights):
    parts = [[None, None] for _ in range(4)]
    for k, weight in enumerate(weights):
        for u in range(4):
            term = weight * source[h, pl.ds(base + k + u * 8, 8), :]
            old = parts[u][k % 2]
            parts[u][k % 2] = term if old is None else old + term
    return [p[0] + p[1] for p in parts]


def conv_rows(glu, taps, conv, start, count):
    n = taps.shape[0]
    for h in range(2):
        weights = [jnp.broadcast_to(taps[k : k + 1, lanes(h)], (8, LANES)) for k in range(n)]

        def step(i, carry, h=h, weights=weights):
            r = start + i * 32
            tiles = weighted(glu, h, r + PAD + 1 - n, weights)
            for u in range(4):
                conv[h, pl.ds(pl.multiple_of(r + u * 8, 8), 8), :] = tiles[u]
            return carry

        lax.fori_loop(0, count // 32, step, 0)


def split(x):
    high = x.astype(BF16)
    return high, (x - high.astype(F32)).astype(BF16)


def selector(row):
    sub = lax.broadcasted_iota(jnp.int32, (8, LANES), 0)
    return (sub == row).astype(F32).astype(BF16)


def row_sums(pairs):
    total = None
    for row, x in pairs:
        pick = selector(row)
        for part in split(x):
            term = lax.dot_general(pick, part, NT, preferred_element_type=F32)
            total = term if total is None else total + term
    return total


def conv_stats(conv, stats, start, count):
    for r in range(start, start + count, 256):
        pairs = []
        for h in range(2):
            c = conv[h, r : r + 256, :]
            pairs += [(0, c), (1, c * c)]
        stats[:, r : r + 256] = row_sums(pairs)


def conv_body(grad_in, weight_in, glu, taps, conv, stats, out_grad, weight, sems):
    rows = conv.shape[1]
    loads = moves(((weight_in, weight), (grad_in, out_grad)), sems)
    conv_rows(glu, taps, conv, PAD, rows - PAD)
    conv_stats(conv, stats, 256, rows - 256)
    for load in loads:
        load.wait()


def head_body(edge, glu_in, taps, conv_in, stats_in, glu, conv, sent, stats):
    for h in range(2):
        glu[h, 0:PAD, :] = edge[h]
    conv_rows(glu, taps, conv, 0, PAD)
    conv_stats(conv, stats, 0, 256)
    rows = conv.shape[1]
    for p in range(sent.shape[0]):
        sent[p, :, 0:256] = stats[0:2]
        sent[p, :, 256:rows] = stats_in[0:2, 256:rows]


def spread(rows, stack, columns):
    stats, length = rows.shape
    blocks = length // LANES
    stack[...] = jnp.zeros(stack.shape, F32)
    for s in range(stats):
        for b in range(blocks):
            stack[s * blocks + b : s * blocks + b + 1, :] = rows[s : s + 1, b * LANES : (b + 1) * LANES]
    turned = stack[...].T
    for s in range(stats):
        for b in range(blocks):
            j = s * blocks + b
            columns[s, b * LANES : (b + 1) * LANES] = jnp.broadcast_to(
                turned[:, j : j + 1], (LANES, LANES)
            )


def norm_body(
    stats, conv, act_grad, gain, activ, xhats, scaled, sums, gain_sum, rows_in, stack, columns
):
    peers = stats.shape[0]
    rows = conv.shape[1]
    channels = 2 * LANES * peers
    total = stats[0]
    for p in range(1, peers):
        total = total + stats[p]
    mean = total[0:1] * (1.0 / channels)
    rows_in[0:1, :] = lax.rsqrt(total[1:2] * (1.0 / channels) - mean * mean + 1e-05)
    rows_in[1:2, :] = mean
    spread(rows_in, stack, columns)
    for h in range(2):
        gain_sum[h] = jnp.zeros((8, LANES), F32)
    size = 256

    def step(j, carry):
        at = pl.ds(pl.multiple_of(j * 128, 128), 128)
        rs, mu = columns[0, at], columns[1, at]
        for h in range(2):
            g = gain[0:1, lanes(h)]
            xhat = (conv[h, at, :] - mu) * rs
            normed = xhat * g
            sig = jax.nn.sigmoid(normed)
            act = normed * sig
            activ[at, lanes(h)] = act.astype(BF16)
            ng = act_grad[at, lanes(h)] * (sig + act * (1.0 - sig))
            gain_sum[h] += jnp.sum((ng * xhat).reshape(16, 8, LANES), axis=0)
            xhats[h, at, :] = xhat
            scaled[h, at, :] = ng * g * rs
        return carry

    lax.fori_loop(0, rows // 128, step, 0)
    for r in range(0, rows, size):
        pairs = []
        for h in range(2):
            x = scaled[h, r : r + size, :]
            pairs += [(0, x), (1, x * xhats[h, r : r + size, :])]
        out = row_sums(pairs)
        for p in range(peers):
            sums[p, :, r : r + size] = out[0:2]


def taps_body(
    n, sent_in, sums, scaled, xhat, glu, gain_sum, grad, sent, rows_in, stack, columns, small
):
    rows = grad.shape[1]
    peers = sums.shape[0]
    total = sums[0]
    for p in range(1, peers):
        total = total + sums[p]
    rows_in[...] = total * (1.0 / (2 * LANES * peers))
    spread(rows_in, stack, columns)

    def step(j, carry):
        at = pl.ds(pl.multiple_of(j * 64, 64), 64)
        for h in range(2):
            grad[h, at, :] = scaled[h, at, :] - columns[0, at] - xhat[h, at, :] * columns[1, at]
        return carry

    lax.fori_loop(0, rows // 64, step, 0)
    for h in range(2):
        for lo, hi in ((0, 16), (16, n)):

            def tile(i, acc, h=h, lo=lo, hi=hi):
                acc = list(acc)
                r = pl.multiple_of(i * 64, 64)
                c = [grad[h, pl.ds(r + u * 8, 8), :] for u in range(8)]
                for u in range(8):
                    for k in range(lo, hi):
                        base = r + PAD + 1 - n + k
                        acc[k - lo] = acc[k - lo] + c[u] * glu[h, pl.ds(base + u * 8, 8), :]
                return tuple(acc)

            zero = tuple(jnp.zeros((8, LANES), F32) for _ in range(lo, hi))
            acc = lax.fori_loop(0, rows // 64, tile, zero)
            for k in range(lo, hi):
                small[k : k + 1, lanes(h)] = jnp.sum(acc[k - lo], axis=0, keepdims=True)
        small[n : n + 1, lanes(h)] = jnp.sum(gain_sum[h], axis=0, keepdims=True)
    top = sent.shape[0] - 8
    for q in range(4):
        sent[top:, 256 * q : 256 * q + 256] = small[8 * q : 8 * q + 8]


def pack_body(kept, sent, received, out):
    rows, outs = kept.shape
    total = sent[rows:] + received[rows:]
    small = jnp.concatenate([total[:, 0:512], total[:, 512:1024]], axis=0).astype(BF16)
    for p in range(out.shape[0]):
        at = slice(p * 16, (p + 1) * 16)
        out[p, :, 0:outs] = (kept[at] + received[at]).astype(BF16)
        out[p, :, outs:] = small


def relay_body(got, out, held):
    outs = got.shape[2] - 512
    total = got[0].astype(F32)
    for p in range(1, got.shape[0]):
        total = total + got[p].astype(F32)
    held[...] = total[:, 0:outs]
    for p in range(out.shape[0]):
        out[p, :, 0:512] = total[0:8, outs:]
        out[p, :, 512:1024] = total[8:16, outs:]
        for i in range(2):
            for j in range(4):
                out[p, 4 * i + j : 4 * i + j + 1, 1024:1280] = held[
                    2 * p + i : 2 * p + i + 1, 256 * j : 256 * j + 256
                ]


def final_body(factor, got, proj, taps, gain):
    total = got[0]
    for p in range(1, got.shape[0]):
        total = total + got[p]
    total = total * factor
    taps[0:8] = total[:, 0:256]
    taps[8:16] = total[:, 256:512]
    taps[16:24] = total[:, 512:768]
    taps[24:31] = total[0:7, 768:1024]
    gain[...] = total[7:8, 768:1024]
    for i in range(2):
        for j in range(4):
            proj[i : i + 1, 256 * j : 256 * j + 256] = total[4 * i + j : 4 * i + j + 1, 1024:1280]


def moves(pairs, sems):
    copies = [pltpu.make_async_copy(x, y, sems.at[k]) for k, (x, y) in enumerate(pairs)]
    for copy in copies:
        copy.start()
    return copies


def glu_grad_rows(source, offset, taps, value, gate, out_value, out_gate, first, count):
    n = taps.shape[0]
    for h in range(2):
        weights = [jnp.broadcast_to(taps[k : k + 1, lanes(h)], (8, LANES)) for k in range(n)]

        def step(i, carry, h=h, weights=weights):
            tiles = weighted(source, h, offset + i * 32, weights[::-1])
            at = pl.ds(pl.multiple_of(first + i * 32, 32), 32)
            sig = jax.nn.sigmoid(gate[at, lanes(h)].astype(F32))
            got = jnp.concatenate(tiles, axis=0) * sig
            out_value[at, lanes(h)] = got.astype(BF16)
            out_gate[at, lanes(h)] = (got * value[at, lanes(h)].astype(F32) * (1.0 - sig)).astype(BF16)
            return carry

        lax.fori_loop(0, count // 32, step, 0)


def glu_head_body(
    value_in, gate_in, grad, taps, value_grad, gate_grad, value, gate, out_value, out_gate, sems
):
    count = value.shape[0]
    at = pl.ds(0, count)
    for copy in moves(((value_in.at[at], value), (gate_in.at[at], gate)), sems):
        copy.wait()
    glu_grad_rows(grad, 0, taps, value, gate, out_value, out_gate, 0, count)
    for copy in moves(((out_value, value_grad.at[at]), (out_gate, gate_grad.at[at])), sems):
        copy.wait()


def glu_tail_body(
    value_in, gate_in, value_part, gate_part, grad, after, taps, value_grad, gate_grad,
    value, gate, out_value, out_gate, ext, sems,
):
    count = value.shape[0]
    rows = grad.shape[1]
    at = pl.ds(rows - count, count)
    loads = moves(((value_in.at[at], value), (gate_in.at[at], gate)), sems)
    for h in range(2):
        ext[h, 0:PAD, :] = grad[h, rows - PAD :, :]
        ext[h, PAD : 2 * PAD, :] = after[h]
    for load in loads:
        load.wait()
    if count > PAD:
        glu_grad_rows(grad, rows - count, taps, value, gate, out_value, out_gate, 0, count - PAD)
    glu_grad_rows(ext, 0, taps, value, gate, out_value, out_gate, count - PAD, PAD)
    for copy in moves(((out_value, value_grad.at[at]), (out_gate, gate_grad.at[at])), sems):
        copy.wait()


def act_body(out_grad, weight, act):
    act[...] = lax.dot_general(out_grad[...], weight[...], NT, preferred_element_type=F32)


def proj_body(me, activ, out_grad, kept, sent):
    width = activ.shape[1]
    half = width // 2
    row = lax.broadcasted_iota(jnp.int32, (width, width), 0)
    col = lax.broadcasted_iota(jnp.int32, (width, width), 1)
    low = jnp.bitwise_and(row, half - 1)
    high = jnp.bitwise_xor(jnp.right_shift(row, 7), me[0])
    source = jnp.left_shift(jnp.right_shift(low, 1), 2) + 2 * high + jnp.bitwise_and(row, 1)
    order = (col == source).astype(F32).astype(BF16)
    placed = lax.dot_general(order, activ[...], NT, preferred_element_type=F32).astype(BF16)
    kept[...] = jnp.dot(placed[:half], out_grad[...], preferred_element_type=F32)
    sent[0:half] = jnp.dot(placed[half:], out_grad[...], preferred_element_type=F32)


def over_tp(array):
    return lax.all_to_all(array, "tp", 0, 0, tiled=True)


def per_device(glu_value, glu_gate, conv_taps, channel_gain, proj_weight, out_grad):
    n = conv_taps.shape[0]
    rows, width = glu_value.shape
    peers = lax.axis_size("tp")
    outs = out_grad.shape[1]
    factor = 1.0 / math.sqrt(rows * lax.axis_size(SP))

    def wide(length):
        return ((2, length, LANES), F32, "near")

    stat = ((peers, 2, rows), F32, "near")
    dma = pltpu.SemaphoreType.DMA
    tall = ((rows, width), BF16)
    glu, edge, taps = kernel(
        glu_body,
        [wide(rows + PAD), wide(PAD), ((n, width), F32, "near")],
        (far(glu_value), far(glu_gate), far(conv_taps)),
        ins=[HBM] * 3,
        scratch=[tall, tall, dma((2, 5))],
    )
    edge = shifted(edge, 1)
    conv, stats, out_grad, weight = kernel(
        conv_body,
        [
            wide(rows),
            ((8, rows), F32, "near"),
            (out_grad.shape, BF16, "near"),
            (proj_weight.shape, BF16, "near"),
        ],
        (far(out_grad), far(proj_weight), near(glu), near(taps)),
        ins=[HBM] * 2,
        scratch=[dma((2,))],
    )
    (act_grad,) = kernel(act_body, [((rows, width), F32, "near")], (near(out_grad), near(weight)))
    me = lax.axis_index("core")[None]
    edge, act_grad, me = lax.optimization_barrier((edge, act_grad, me))
    glu, conv, stats = kernel(
        head_body,
        [wide(rows + PAD), wide(rows), stat],
        (near(edge), near(glu), near(taps), near(conv), near(stats)),
        aliases={1: 0, 3: 1},
        scratch=[((8, 256), F32)],
    )
    stats = over_tp(stats)
    spreading = [((2, rows), F32), ((LANES, LANES), F32), ((2, rows, LANES), F32)]
    activ, xhat, scaled, sums, gain_sum = kernel(
        norm_body,
        [(*tall, "near"), wide(rows), wide(rows), stat, wide(8)],
        (near(stats), near(conv), near(act_grad), channel_gain[None]),
        scratch=spreading,
    )
    sums = over_tp(sums)
    sums, activ = lax.optimization_barrier((sums, activ))
    joint = ((width // 2 + 8, outs), F32, "near")
    kept, sent = kernel(
        proj_body,
        [((width // 2, outs), F32, "near"), joint],
        (me, near(activ), near(out_grad)),
        ins=[SMEM],
    )
    grad, sent = kernel(
        lambda *refs: taps_body(n, *refs),
        [wide(rows), joint],
        (near(sent), near(sums), near(scaled), near(xhat), near(glu), near(gain_sum)),
        aliases={0: 1},
        scratch=[*spreading, ((32, width), F32)],
    )
    received = swapped(sent)
    (first,) = kernel(
        pack_body, [((8, 16, outs + 512), BF16, "any")], (near(kept), near(sent), near(received))
    )
    first = lax.all_to_all(first, "z", 0, 0, tiled=True)
    after = shifted(grad[:, :PAD], -1)

    def gates(length):
        return [((length, width), BF16)] * 4

    value_grad, gate_grad = kernel(
        glu_head_body,
        [(*tall, "far")] * 2,
        (far(glu_value), far(glu_gate), near(grad), conv_taps),
        ins=[HBM] * 2,
        out_specs=[HBM] * 2,
        scratch=[*gates(rows // 2), dma((2,))],
    )
    first, after, value_grad, gate_grad = lax.optimization_barrier((first, after, value_grad, gate_grad))
    (second,) = kernel(
        relay_body, [((8, 8, 1280), F32, "any")], (near(first),), scratch=[((16, outs), F32)]
    )
    second = lax.all_to_all(second, "y", 0, 0, tiled=True)
    value_grad, gate_grad = kernel(
        glu_tail_body,
        [(*tall, "far")] * 2,
        (
            far(glu_value), far(glu_gate), far(value_grad), far(gate_grad), near(grad),
            near(after), conv_taps,
        ),
        ins=[HBM] * 4,
        out_specs=[HBM] * 2,
        aliases={2: 0, 3: 1},
        scratch=[*gates(rows // 2), ((2, 2 * PAD, LANES), F32), dma((2,))],
    )
    second, value_grad, gate_grad = lax.optimization_barrier((second, value_grad, gate_grad))
    proj_grad, taps_grad, gain_grad = kernel(
        lambda *refs: final_body(factor, *refs),
        [((2, outs), F32, "any"), ((n, width), F32, "any"), ((1, width), F32, "any")],
        (near(second),),
    )
    return (value_grad, gate_grad, proj_grad, taps_grad, gain_grad.reshape(width))


def solution(mesh):
    finer = Mesh(mesh.devices.reshape(8, 8, 2, mesh.shape["tp"]), (*SP, "tp"))
    return jax.shard_map(
        per_device,
        mesh=finer,
        in_specs=(P(SP, "tp"), P(SP, "tp"), P(None, "tp"), P("tp"), P("tp", None), P(SP, None)),
        out_specs=(P(SP, "tp"), P(SP, "tp"), P(("tp", *SP), None), P(None, "tp"), P("tp")),
        check_vma=False,
    )
```

```python
import math

import jax
import jax.numpy as jnp
from jax import lax
from jax.experimental import pallas as pl
from jax.experimental.pallas import tpu as pltpu
from jax.sharding import Mesh
from jax.sharding import PartitionSpec as P


SP = ("z", "y", "core")
Y_ORDER = [4, 5, 6, 7, 0, 1, 2, 3]
F32, BF16 = jnp.float32, jnp.bfloat16
LANES = 128
PAD = 32
NT = (((1,), (1,)), ((), ()))


def shifted(block, distance):
    devices = range(lax.axis_size(SP))
    route = [(i - distance, i) for i in devices if i - distance in devices]
    return lax.ppermute(block, SP, route)


def swapped(block):
    return lax.ppermute(block, "core", [(0, 1), (1, 0)])


def near(array):
    return pltpu.with_memory_space_constraint(array, pltpu.VMEM)


def far(array):
    return pltpu.with_memory_space_constraint(array, pltpu.HBM)


VMEM, HBM, SMEM = (pl.BlockSpec(memory_space=m) for m in (pltpu.VMEM, pltpu.HBM, pltpu.SMEM))


def kernel(body, outs, args, ins=(), out_specs=None, scratch=(), aliases=None, limit=16):
    shapes = {
        "near": pltpu.VMEM,
        "far": pltpu.HBM,
        "any": jax.ShapeDtypeStruct,
    }
    return pl.pallas_call(
        body,
        out_shape=[shapes[where](s, d) for s, d, where in outs],
        in_specs=list(ins) + [VMEM] * (len(args) - len(ins)),
        out_specs=out_specs or [VMEM] * len(outs),
        scratch_shapes=[pltpu.VMEM(*x) if isinstance(x, tuple) else x for x in scratch],
        input_output_aliases=aliases or {},
        compiler_params=pltpu.CompilerParams(vmem_limit_bytes=limit << 20),
    )(*args)


def lanes(h):
    return slice(h * LANES, (h + 1) * LANES)


def glu_body(value_in, gate_in, taps_in, glu, edge, taps, value, gate, sems):
    rows = value.shape[0]
    chunks = sems.shape[1] - 1
    size = rows // chunks
    load_taps = pltpu.make_async_copy(taps_in, taps, sems.at[0, chunks])
    loads = []
    for c in range(chunks):
        at = pl.ds(c * size, size)
        loads.append(pltpu.make_async_copy(value_in.at[at], value.at[at], sems.at[0, c]))
        loads.append(pltpu.make_async_copy(gate_in.at[at], gate.at[at], sems.at[1, c]))
    for load in loads:
        load.start()
    load_taps.start()
    for c in range(chunks):
        loads[2 * c].wait()
        loads[2 * c + 1].wait()

        def step(i, carry, c=c):
            r = pl.multiple_of(c * size + i * 64, 64)
            for h in range(2):
                v = value[pl.ds(r, 64), lanes(h)].astype(F32)
                g = gate[pl.ds(r, 64), lanes(h)].astype(F32)
                glu[h, pl.ds(PAD + r, 64), :] = v * jax.nn.sigmoid(g)
            return carry

        lax.fori_loop(0, size // 64, step, 0)
    for h in range(2):
        edge[h] = glu[h, rows : rows + PAD, :]
    load_taps.wait()


def weighted(source, h, base, weights):
    parts = [[None, None] for _ in range(4)]
    for k, weight in enumerate(weights):
        for u in range(4):
            term = weight * source[h, pl.ds(base + k + u * 8, 8), :]
            old = parts[u][k % 2]
            parts[u][k % 2] = term if old is None else old + term
    return [p[0] + p[1] for p in parts]


def conv_rows(glu, taps, conv, start, count):
    n = taps.shape[0]
    for h in range(2):
        weights = [jnp.broadcast_to(taps[k : k + 1, lanes(h)], (8, LANES)) for k in range(n)]

        def step(i, carry, h=h, weights=weights):
            r = start + i * 32
            tiles = weighted(glu, h, r + PAD + 1 - n, weights)
            for u in range(4):
                conv[h, pl.ds(pl.multiple_of(r + u * 8, 8), 8), :] = tiles[u]
            return carry

        lax.fori_loop(0, count // 32, step, 0)


def split(x):
    high = x.astype(BF16)
    return high, (x - high.astype(F32)).astype(BF16)


def selector(row):
    sub = lax.broadcasted_iota(jnp.int32, (8, LANES), 0)
    return (sub == row).astype(F32).astype(BF16)


def row_sums(pairs):
    total = None
    for row, x in pairs:
        pick = selector(row)
        for part in split(x):
            term = lax.dot_general(pick, part, NT, preferred_element_type=F32)
            total = term if total is None else total + term
    return total


def conv_stats(conv, stats, start, count):
    for r in range(start, start + count, 256):
        pairs = []
        for h in range(2):
            c = conv[h, r : r + 256, :]
            pairs += [(0, c), (1, c * c)]
        stats[:, r : r + 256] = row_sums(pairs)


def conv_body(grad_in, weight_in, glu, taps, conv, stats, out_grad, weight, sems):
    rows = conv.shape[1]
    loads = moves(((weight_in, weight), (grad_in, out_grad)), sems)
    conv_rows(glu, taps, conv, PAD, rows - PAD)
    conv_stats(conv, stats, 256, rows - 256)
    for load in loads:
        load.wait()


def head_body(edge, glu_in, taps, conv_in, stats_in, glu, conv, sent, stats):
    for h in range(2):
        glu[h, 0:PAD, :] = edge[h]
    conv_rows(glu, taps, conv, 0, PAD)
    conv_stats(conv, stats, 0, 256)
    rows = conv.shape[1]
    for p in range(sent.shape[0]):
        sent[p, :, 0:256] = stats[0:2]
        sent[p, :, 256:rows] = stats_in[0:2, 256:rows]


def spread(rows, stack, columns):
    stats, length = rows.shape
    blocks = length // LANES
    stack[...] = jnp.zeros(stack.shape, F32)
    for s in range(stats):
        for b in range(blocks):
            stack[s * blocks + b : s * blocks + b + 1, :] = rows[s : s + 1, b * LANES : (b + 1) * LANES]
    turned = stack[...].T
    for s in range(stats):
        for b in range(blocks):
            j = s * blocks + b
            columns[s, b * LANES : (b + 1) * LANES] = jnp.broadcast_to(
                turned[:, j : j + 1], (LANES, LANES)
            )


def norm_body(
    stats, conv, act_grad, gain, activ, xhats, scaled, sums, gain_sum, rows_in, stack, columns
):
    peers = stats.shape[0]
    rows = conv.shape[1]
    channels = 2 * LANES * peers
    total = stats[0]
    for p in range(1, peers):
        total = total + stats[p]
    mean = total[0:1] * (1.0 / channels)
    rows_in[0:1, :] = lax.rsqrt(total[1:2] * (1.0 / channels) - mean * mean + 1e-05)
    rows_in[1:2, :] = mean
    spread(rows_in, stack, columns)
    for h in range(2):
        gain_sum[h] = jnp.zeros((8, LANES), F32)
    size = 256

    def step(j, carry):
        at = pl.ds(pl.multiple_of(j * 128, 128), 128)
        rs, mu = columns[0, at], columns[1, at]
        for h in range(2):
            g = gain[0:1, lanes(h)]
            xhat = (conv[h, at, :] - mu) * rs
            normed = xhat * g
            sig = jax.nn.sigmoid(normed)
            act = normed * sig
            activ[at, lanes(h)] = act.astype(BF16)
            ng = act_grad[at, lanes(h)] * (sig + act * (1.0 - sig))
            gain_sum[h] += jnp.sum((ng * xhat).reshape(16, 8, LANES), axis=0)
            xhats[h, at, :] = xhat
            scaled[h, at, :] = ng * g * rs
        return carry

    lax.fori_loop(0, rows // 128, step, 0)
    for r in range(0, rows, size):
        pairs = []
        for h in range(2):
            x = scaled[h, r : r + size, :]
            pairs += [(0, x), (1, x * xhats[h, r : r + size, :])]
        out = row_sums(pairs)
        for p in range(peers):
            sums[p, :, r : r + size] = out[0:2]


def taps_body(
    n, sent_in, sums, scaled, xhat, glu, gain_sum, grad, sent, rows_in, stack, columns, small
):
    rows = grad.shape[1]
    peers = sums.shape[0]
    total = sums[0]
    for p in range(1, peers):
        total = total + sums[p]
    rows_in[...] = total * (1.0 / (2 * LANES * peers))
    spread(rows_in, stack, columns)

    def step(j, carry):
        at = pl.ds(pl.multiple_of(j * 64, 64), 64)
        for h in range(2):
            grad[h, at, :] = scaled[h, at, :] - columns[0, at] - xhat[h, at, :] * columns[1, at]
        return carry

    lax.fori_loop(0, rows // 64, step, 0)
    for h in range(2):
        for lo, hi in ((0, 16), (16, n)):

            def tile(i, acc, h=h, lo=lo, hi=hi):
                acc = list(acc)
                r = pl.multiple_of(i * 128, 128)
                c = [grad[h, pl.ds(r + u * 8, 8), :] for u in range(16)]
                for u in range(16):
                    for k in range(lo, hi):
                        base = r + PAD + 1 - n + k
                        acc[k - lo] = acc[k - lo] + c[u] * glu[h, pl.ds(base + u * 8, 8), :]
                return tuple(acc)

            zero = tuple(jnp.zeros((8, LANES), F32) for _ in range(lo, hi))
            acc = lax.fori_loop(0, rows // 128, tile, zero)
            for k in range(lo, hi):
                small[k : k + 1, lanes(h)] = jnp.sum(acc[k - lo], axis=0, keepdims=True)
        small[n : n + 1, lanes(h)] = jnp.sum(gain_sum[h], axis=0, keepdims=True)
    top = sent.shape[0] - 8
    for q in range(4):
        sent[top:, 256 * q : 256 * q + 256] = small[8 * q : 8 * q + 8]


def pack_body(kept, sent, received, out):
    rows, outs = kept.shape
    total = sent[rows:] + received[rows:]
    small = jnp.concatenate([total[:, 0:512], total[:, 512:1024]], axis=0).astype(BF16)
    for p in range(out.shape[0]):
        at = slice(p * 16, (p + 1) * 16)
        out[p, :, 0:outs] = (kept[at] + received[at]).astype(BF16)
        out[p, :, outs:] = small


def relay_body(got, out, held):
    outs = got.shape[2] - 512
    total = got[0].astype(F32)
    for p in range(1, got.shape[0]):
        total = total + got[p].astype(F32)
    held[...] = total[:, 0:outs]
    for p in range(out.shape[0]):
        out[p, :, 0:512] = total[0:8, outs:]
        out[p, :, 512:1024] = total[8:16, outs:]
        for i in range(2):
            for j in range(4):
                out[p, 4 * i + j : 4 * i + j + 1, 1024:1280] = held[
                    2 * Y_ORDER[p] + i : 2 * Y_ORDER[p] + i + 1, 256 * j : 256 * j + 256
                ]


def final_body(factor, got, proj, taps, gain):
    total = got[0]
    for p in range(1, got.shape[0]):
        total = total + got[p]
    total = total * factor
    taps[0:8] = total[:, 0:256]
    taps[8:16] = total[:, 256:512]
    taps[16:24] = total[:, 512:768]
    taps[24:31] = total[0:7, 768:1024]
    gain[...] = total[7:8, 768:1024]
    for i in range(2):
        for j in range(4):
            proj[i : i + 1, 256 * j : 256 * j + 256] = total[4 * i + j : 4 * i + j + 1, 1024:1280]


def moves(pairs, sems):
    copies = [pltpu.make_async_copy(x, y, sems.at[k]) for k, (x, y) in enumerate(pairs)]
    for copy in copies:
        copy.start()
    return copies


def glu_grad_rows(source, offset, taps, value, gate, out_value, out_gate, first, count):
    n = taps.shape[0]
    for h in range(2):
        weights = [jnp.broadcast_to(taps[k : k + 1, lanes(h)], (8, LANES)) for k in range(n)]

        def step(i, carry, h=h, weights=weights):
            tiles = weighted(source, h, offset + i * 32, weights[::-1])
            at = pl.ds(pl.multiple_of(first + i * 32, 32), 32)
            sig = jax.nn.sigmoid(gate[at, lanes(h)].astype(F32))
            got = jnp.concatenate(tiles, axis=0) * sig
            out_value[at, lanes(h)] = got.astype(BF16)
            out_gate[at, lanes(h)] = (got * value[at, lanes(h)].astype(F32) * (1.0 - sig)).astype(BF16)
            return carry

        lax.fori_loop(0, count // 32, step, 0)


def glu_head_body(
    value_in, gate_in, grad, taps, value_grad, gate_grad, value, gate, out_value, out_gate, sems
):
    count = value.shape[0]
    at = pl.ds(0, count)
    for copy in moves(((value_in.at[at], value), (gate_in.at[at], gate)), sems):
        copy.wait()
    glu_grad_rows(grad, 0, taps, value, gate, out_value, out_gate, 0, count)
    for copy in moves(((out_value, value_grad.at[at]), (out_gate, gate_grad.at[at])), sems):
        copy.wait()


def glu_tail_body(
    value_in, gate_in, value_part, gate_part, grad, after, taps, value_grad, gate_grad,
    value, gate, out_value, out_gate, ext, sems,
):
    count = value.shape[0]
    rows = grad.shape[1]
    at = pl.ds(rows - count, count)
    loads = moves(((value_in.at[at], value), (gate_in.at[at], gate)), sems)
    for h in range(2):
        ext[h, 0:PAD, :] = grad[h, rows - PAD :, :]
        ext[h, PAD : 2 * PAD, :] = after[h]
    for load in loads:
        load.wait()
    if count > PAD:
        glu_grad_rows(grad, rows - count, taps, value, gate, out_value, out_gate, 0, count - PAD)
    glu_grad_rows(ext, 0, taps, value, gate, out_value, out_gate, count - PAD, PAD)
    for copy in moves(((out_value, value_grad.at[at]), (out_gate, gate_grad.at[at])), sems):
        copy.wait()


def act_body(out_grad, weight, act):
    act[...] = lax.dot_general(out_grad[...], weight[...], NT, preferred_element_type=F32)


def proj_body(me, activ, out_grad, kept, sent):
    width = activ.shape[1]
    half = width // 2
    row = lax.broadcasted_iota(jnp.int32, (width, width), 0)
    col = lax.broadcasted_iota(jnp.int32, (width, width), 1)
    low = jnp.bitwise_and(row, half - 1)
    high = jnp.bitwise_xor(jnp.right_shift(row, 7), me[0])
    source = jnp.left_shift(jnp.right_shift(low, 1), 2) + 2 * high + jnp.bitwise_and(row, 1)
    order = (col == source).astype(F32).astype(BF16)
    placed = lax.dot_general(order, activ[...], NT, preferred_element_type=F32).astype(BF16)
    kept[...] = jnp.dot(placed[:half], out_grad[...], preferred_element_type=F32)
    sent[0:half] = jnp.dot(placed[half:], out_grad[...], preferred_element_type=F32)


def over_tp(array):
    return lax.all_to_all(array, "tp", 0, 0, tiled=True)


def per_device(glu_value, glu_gate, conv_taps, channel_gain, proj_weight, out_grad):
    n = conv_taps.shape[0]
    rows, width = glu_value.shape
    peers = lax.axis_size("tp")
    outs = out_grad.shape[1]
    factor = 1.0 / math.sqrt(rows * lax.axis_size(SP))

    def wide(length):
        return ((2, length, LANES), F32, "near")

    stat = ((peers, 2, rows), F32, "near")
    dma = pltpu.SemaphoreType.DMA
    tall = ((rows, width), BF16)
    glu, edge, taps = kernel(
        glu_body,
        [wide(rows + PAD), wide(PAD), ((n, width), F32, "near")],
        (far(glu_value), far(glu_gate), far(conv_taps)),
        ins=[HBM] * 3,
        scratch=[tall, tall, dma((2, 5))],
    )
    edge = shifted(edge, 1)
    conv, stats, out_grad, weight = kernel(
        conv_body,
        [
            wide(rows),
            ((8, rows), F32, "near"),
            (out_grad.shape, BF16, "near"),
            (proj_weight.shape, BF16, "near"),
        ],
        (far(out_grad), far(proj_weight), near(glu), near(taps)),
        ins=[HBM] * 2,
        scratch=[dma((2,))],
    )
    (act_grad,) = kernel(act_body, [((rows, width), F32, "near")], (near(out_grad), near(weight)))
    me = lax.axis_index("core")[None]
    edge, act_grad, me = lax.optimization_barrier((edge, act_grad, me))
    glu, conv, stats = kernel(
        head_body,
        [wide(rows + PAD), wide(rows), stat],
        (near(edge), near(glu), near(taps), near(conv), near(stats)),
        aliases={1: 0, 3: 1},
        scratch=[((8, 256), F32)],
    )
    stats = over_tp(stats)
    spreading = [((2, rows), F32), ((LANES, LANES), F32), ((2, rows, LANES), F32)]
    activ, xhat, scaled, sums, gain_sum = kernel(
        norm_body,
        [(*tall, "near"), wide(rows), wide(rows), stat, wide(8)],
        (near(stats), near(conv), near(act_grad), channel_gain[None]),
        scratch=spreading,
    )
    sums = over_tp(sums)
    sums, activ = lax.optimization_barrier((sums, activ))
    joint = ((width // 2 + 8, outs), F32, "near")
    kept, sent = kernel(
        proj_body,
        [((width // 2, outs), F32, "near"), joint],
        (me, near(activ), near(out_grad)),
        ins=[SMEM],
    )
    grad, sent = kernel(
        lambda *refs: taps_body(n, *refs),
        [wide(rows), joint],
        (near(sent), near(sums), near(scaled), near(xhat), near(glu), near(gain_sum)),
        aliases={0: 1},
        scratch=[*spreading, ((32, width), F32)],
    )
    received = swapped(sent)
    (first,) = kernel(
        pack_body, [((8, 16, outs + 512), BF16, "any")], (near(kept), near(sent), near(received))
    )
    first = lax.all_to_all(first, "z", 0, 0, tiled=True)
    after = shifted(grad[:, :PAD], -1)

    def gates(length):
        return [((length, width), BF16)] * 4

    value_grad, gate_grad = kernel(
        glu_head_body,
        [(*tall, "far")] * 2,
        (far(glu_value), far(glu_gate), near(grad), conv_taps),
        ins=[HBM] * 2,
        out_specs=[HBM] * 2,
        scratch=[*gates(rows // 2), dma((2,))],
    )
    first, after, value_grad, gate_grad = lax.optimization_barrier((first, after, value_grad, gate_grad))
    (second,) = kernel(
        relay_body, [((8, 8, 1280), F32, "any")], (near(first),), scratch=[((16, outs), F32)]
    )
    second = lax.all_to_all(second, "y", 0, 0, tiled=True, axis_index_groups=[Y_ORDER])
    value_grad, gate_grad = kernel(
        glu_tail_body,
        [(*tall, "far")] * 2,
        (
            far(glu_value), far(glu_gate), far(value_grad), far(gate_grad), near(grad),
            near(after), conv_taps,
        ),
        ins=[HBM] * 4,
        out_specs=[HBM] * 2,
        aliases={2: 0, 3: 1},
        scratch=[*gates(rows // 2), ((2, 2 * PAD, LANES), F32), dma((2,))],
    )
    second, value_grad, gate_grad = lax.optimization_barrier((second, value_grad, gate_grad))
    proj_grad, taps_grad, gain_grad = kernel(
        lambda *refs: final_body(factor, *refs),
        [((2, outs), F32, "any"), ((n, width), F32, "any"), ((1, width), F32, "any")],
        (near(second),),
    )
    return (value_grad, gate_grad, proj_grad, taps_grad, gain_grad.reshape(width))


def solution(mesh):
    finer = Mesh(mesh.devices.reshape(8, 8, 2, mesh.shape["tp"]), (*SP, "tp"))
    return jax.shard_map(
        per_device,
        mesh=finer,
        in_specs=(P(SP, "tp"), P(SP, "tp"), P(None, "tp"), P("tp"), P("tp", None), P(SP, None)),
        out_specs=(P(SP, "tp"), P(SP, "tp"), P(("tp", *SP), None), P(None, "tp"), P("tp")),
        check_vma=False,
    )
```

```python
import math

import jax
import jax.numpy as jnp
from jax import lax
from jax.experimental import pallas as pl
from jax.experimental.pallas import tpu as pltpu
from jax.sharding import Mesh
from jax.sharding import PartitionSpec as P


SP = ("z", "y", "core")
X_ORDER = [3, 0, 1, 2]
Y_ORDER = [4, 5, 6, 7, 0, 1, 2, 3]
Z_ORDER = [4, 5, 6, 7, 0, 1, 2, 3]
F32, BF16 = jnp.float32, jnp.bfloat16
LANES = 128
PAD = 32
NT = (((1,), (1,)), ((), ()))


def shifted(block, distance):
    devices = range(lax.axis_size(SP))
    route = [(i - distance, i) for i in devices if i - distance in devices]
    return lax.ppermute(block, SP, route)


def swapped(block):
    return lax.ppermute(block, "core", [(0, 1), (1, 0)])


def near(array):
    return pltpu.with_memory_space_constraint(array, pltpu.VMEM)


def far(array):
    return pltpu.with_memory_space_constraint(array, pltpu.HBM)


VMEM, HBM, SMEM = (pl.BlockSpec(memory_space=m) for m in (pltpu.VMEM, pltpu.HBM, pltpu.SMEM))


def kernel(body, outs, args, ins=(), out_specs=None, scratch=(), aliases=None, limit=16):
    shapes = {
        "near": pltpu.VMEM,
        "far": pltpu.HBM,
        "any": jax.ShapeDtypeStruct,
    }
    return pl.pallas_call(
        body,
        out_shape=[shapes[where](s, d) for s, d, where in outs],
        in_specs=list(ins) + [VMEM] * (len(args) - len(ins)),
        out_specs=out_specs or [VMEM] * len(outs),
        scratch_shapes=[pltpu.VMEM(*x) if isinstance(x, tuple) else x for x in scratch],
        input_output_aliases=aliases or {},
        compiler_params=pltpu.CompilerParams(vmem_limit_bytes=limit << 20),
    )(*args)


def lanes(h):
    return slice(h * LANES, (h + 1) * LANES)


def glu_body(value_in, gate_in, taps_in, glu, edge, taps, value, gate, sems):
    rows = value.shape[0]
    chunks = sems.shape[1] - 1
    size = rows // chunks
    load_taps = pltpu.make_async_copy(taps_in, taps, sems.at[0, chunks])
    loads = []
    for c in range(chunks):
        at = pl.ds(c * size, size)
        loads.append(pltpu.make_async_copy(value_in.at[at], value.at[at], sems.at[0, c]))
        loads.append(pltpu.make_async_copy(gate_in.at[at], gate.at[at], sems.at[1, c]))
    for load in loads:
        load.start()
    load_taps.start()
    for c in range(chunks):
        loads[2 * c].wait()
        loads[2 * c + 1].wait()

        def step(i, carry, c=c):
            r = pl.multiple_of(c * size + i * 64, 64)
            for h in range(2):
                v = value[pl.ds(r, 64), lanes(h)].astype(F32)
                g = gate[pl.ds(r, 64), lanes(h)].astype(F32)
                glu[h, pl.ds(PAD + r, 64), :] = v * jax.nn.sigmoid(g)
            return carry

        lax.fori_loop(0, size // 64, step, 0)
    for h in range(2):
        edge[h] = glu[h, rows : rows + PAD, :]
    load_taps.wait()


def weighted(source, h, base, weights):
    parts = [[None, None] for _ in range(4)]
    for k, weight in enumerate(weights):
        for u in range(4):
            term = weight * source[h, pl.ds(base + k + u * 8, 8), :]
            old = parts[u][k % 2]
            parts[u][k % 2] = term if old is None else old + term
    return [p[0] + p[1] for p in parts]


def conv_rows(glu, taps, conv, start, count):
    n = taps.shape[0]
    for h in range(2):
        weights = [jnp.broadcast_to(taps[k : k + 1, lanes(h)], (8, LANES)) for k in range(n)]

        def step(i, carry, h=h, weights=weights):
            r = start + i * 32
            tiles = weighted(glu, h, r + PAD + 1 - n, weights)
            for u in range(4):
                conv[h, pl.ds(pl.multiple_of(r + u * 8, 8), 8), :] = tiles[u]
            return carry

        lax.fori_loop(0, count // 32, step, 0)


def split(x):
    high = x.astype(BF16)
    return high, (x - high.astype(F32)).astype(BF16)


def selector(row):
    sub = lax.broadcasted_iota(jnp.int32, (8, LANES), 0)
    return (sub == row).astype(F32).astype(BF16)


def row_sums(pairs):
    total = None
    for row, x in pairs:
        pick = selector(row)
        for part in split(x):
            term = lax.dot_general(pick, part, NT, preferred_element_type=F32)
            total = term if total is None else total + term
    return total


def conv_stats(conv, stats, start, count):
    for r in range(start, start + count, 256):
        pairs = []
        for h in range(2):
            c = conv[h, r : r + 256, :]
            pairs += [(0, c), (1, c * c)]
        stats[:, r : r + 256] = row_sums(pairs)


def conv_body(grad_in, weight_in, glu, taps, conv, stats, out_grad, weight, sems):
    rows = conv.shape[1]
    loads = moves(((weight_in, weight), (grad_in, out_grad)), sems)
    conv_rows(glu, taps, conv, PAD, rows - PAD)
    conv_stats(conv, stats, 256, rows - 256)
    for load in loads:
        load.wait()


def head_body(edge, glu_in, taps, conv_in, stats_in, glu, conv, sent, stats):
    for h in range(2):
        glu[h, 0:PAD, :] = edge[h]
    conv_rows(glu, taps, conv, 0, PAD)
    conv_stats(conv, stats, 0, 256)
    rows = conv.shape[1]
    for p in range(sent.shape[0]):
        sent[p, :, 0:256] = stats[0:2]
        sent[p, :, 256:rows] = stats_in[0:2, 256:rows]


def spread(rows, stack, columns):
    stats, length = rows.shape
    blocks = length // LANES
    stack[...] = jnp.zeros(stack.shape, F32)
    for s in range(stats):
        for b in range(blocks):
            stack[s * blocks + b : s * blocks + b + 1, :] = rows[s : s + 1, b * LANES : (b + 1) * LANES]
    turned = stack[...].T
    for s in range(stats):
        for b in range(blocks):
            j = s * blocks + b
            columns[s, b * LANES : (b + 1) * LANES] = jnp.broadcast_to(
                turned[:, j : j + 1], (LANES, LANES)
            )


def norm_body(
    stats, conv, act_grad, gain, activ, xhats, scaled, sums, gain_sum, rows_in, stack, columns
):
    peers = stats.shape[0]
    rows = conv.shape[1]
    channels = 2 * LANES * peers
    total = stats[0]
    for p in range(1, peers):
        total = total + stats[p]
    mean = total[0:1] * (1.0 / channels)
    rows_in[0:1, :] = lax.rsqrt(total[1:2] * (1.0 / channels) - mean * mean + 1e-05)
    rows_in[1:2, :] = mean
    spread(rows_in, stack, columns)
    for h in range(2):
        gain_sum[h] = jnp.zeros((8, LANES), F32)
    size = 256

    def step(j, carry):
        at = pl.ds(pl.multiple_of(j * 128, 128), 128)
        rs, mu = columns[0, at], columns[1, at]
        for h in range(2):
            g = gain[0:1, lanes(h)]
            xhat = (conv[h, at, :] - mu) * rs
            normed = xhat * g
            sig = jax.nn.sigmoid(normed)
            act = normed * sig
            activ[at, lanes(h)] = act.astype(BF16)
            ng = act_grad[at, lanes(h)] * (sig + act * (1.0 - sig))
            gain_sum[h] += jnp.sum((ng * xhat).reshape(16, 8, LANES), axis=0)
            xhats[h, at, :] = xhat
            scaled[h, at, :] = ng * g * rs
        return carry

    lax.fori_loop(0, rows // 128, step, 0)
    for r in range(0, rows, size):
        pairs = []
        for h in range(2):
            x = scaled[h, r : r + size, :]
            pairs += [(0, x), (1, x * xhats[h, r : r + size, :])]
        out = row_sums(pairs)
        for p in range(peers):
            sums[p, :, r : r + size] = out[0:2]


def taps_body(
    n, sent_in, sums, scaled, xhat, glu, gain_sum, grad, sent, rows_in, stack, columns, small
):
    rows = grad.shape[1]
    peers = sums.shape[0]
    total = sums[0]
    for p in range(1, peers):
        total = total + sums[p]
    rows_in[...] = total * (1.0 / (2 * LANES * peers))
    spread(rows_in, stack, columns)

    def step(j, carry):
        at = pl.ds(pl.multiple_of(j * 64, 64), 64)
        for h in range(2):
            grad[h, at, :] = scaled[h, at, :] - columns[0, at] - xhat[h, at, :] * columns[1, at]
        return carry

    lax.fori_loop(0, rows // 64, step, 0)
    for h in range(2):
        for lo, hi in ((0, 16), (16, n)):

            def tile(i, acc, h=h, lo=lo, hi=hi):
                acc = list(acc)
                r = pl.multiple_of(i * 128, 128)
                c = [grad[h, pl.ds(r + u * 8, 8), :] for u in range(16)]
                for u in range(16):
                    for k in range(lo, hi):
                        base = r + PAD + 1 - n + k
                        acc[k - lo] = acc[k - lo] + c[u] * glu[h, pl.ds(base + u * 8, 8), :]
                return tuple(acc)

            zero = tuple(jnp.zeros((8, LANES), F32) for _ in range(lo, hi))
            acc = lax.fori_loop(0, rows // 128, tile, zero)
            for k in range(lo, hi):
                small[k : k + 1, lanes(h)] = jnp.sum(acc[k - lo], axis=0, keepdims=True)
        small[n : n + 1, lanes(h)] = jnp.sum(gain_sum[h], axis=0, keepdims=True)
    top = sent.shape[0] - 8
    for q in range(4):
        sent[top:, 256 * q : 256 * q + 256] = small[8 * q : 8 * q + 8]


def pack_body(kept, sent, received, out):
    rows, outs = kept.shape
    total = sent[rows:] + received[rows:]
    small = jnp.concatenate([total[:, 0:512], total[:, 512:1024]], axis=0).astype(BF16)
    for p, z in enumerate(Z_ORDER):
        at = slice(z * 16, (z + 1) * 16)
        out[p, :, 0:outs] = (kept[at] + received[at]).astype(BF16)
        out[p, :, outs:] = small


def relay_body(got, out, held):
    outs = got.shape[2] - 512
    total = got[0].astype(F32)
    for p in range(1, got.shape[0]):
        total = total + got[p].astype(F32)
    held[...] = total[:, 0:outs]
    for p in range(out.shape[0]):
        out[p, :, 0:512] = total[0:8, outs:]
        out[p, :, 512:1024] = total[8:16, outs:]
        for i in range(2):
            for j in range(4):
                out[p, 4 * i + j : 4 * i + j + 1, 1024:1280] = held[
                    2 * Y_ORDER[p] + i : 2 * Y_ORDER[p] + i + 1, 256 * j : 256 * j + 256
                ]


def final_body(factor, got, proj, taps, gain):
    total = got[0]
    for p in range(1, got.shape[0]):
        total = total + got[p]
    total = total * factor
    taps[0:8] = total[:, 0:256]
    taps[8:16] = total[:, 256:512]
    taps[16:24] = total[:, 512:768]
    taps[24:31] = total[0:7, 768:1024]
    gain[...] = total[7:8, 768:1024]
    for i in range(2):
        for j in range(4):
            proj[i : i + 1, 256 * j : 256 * j + 256] = total[4 * i + j : 4 * i + j + 1, 1024:1280]


def moves(pairs, sems):
    copies = [pltpu.make_async_copy(x, y, sems.at[k]) for k, (x, y) in enumerate(pairs)]
    for copy in copies:
        copy.start()
    return copies


def glu_grad_rows(source, offset, taps, value, gate, out_value, out_gate, first, count):
    n = taps.shape[0]
    for h in range(2):
        weights = [jnp.broadcast_to(taps[k : k + 1, lanes(h)], (8, LANES)) for k in range(n)]

        def step(i, carry, h=h, weights=weights):
            tiles = weighted(source, h, offset + i * 32, weights[::-1])
            at = pl.ds(pl.multiple_of(first + i * 32, 32), 32)
            sig = jax.nn.sigmoid(gate[at, lanes(h)].astype(F32))
            got = jnp.concatenate(tiles, axis=0) * sig
            out_value[at, lanes(h)] = got.astype(BF16)
            out_gate[at, lanes(h)] = (got * value[at, lanes(h)].astype(F32) * (1.0 - sig)).astype(BF16)
            return carry

        lax.fori_loop(0, count // 32, step, 0)


def glu_head_body(
    value_in, gate_in, grad, taps, value_grad, gate_grad, value, gate, out_value, out_gate, sems
):
    count = value.shape[0]
    at = pl.ds(0, count)
    for copy in moves(((value_in.at[at], value), (gate_in.at[at], gate)), sems):
        copy.wait()
    glu_grad_rows(grad, 0, taps, value, gate, out_value, out_gate, 0, count)
    for copy in moves(((out_value, value_grad.at[at]), (out_gate, gate_grad.at[at])), sems):
        copy.wait()


def glu_tail_body(
    value_in, gate_in, value_part, gate_part, grad, after, taps, value_grad, gate_grad,
    value, gate, out_value, out_gate, ext, sems,
):
    count = value.shape[0]
    rows = grad.shape[1]
    at = pl.ds(rows - count, count)
    loads = moves(((value_in.at[at], value), (gate_in.at[at], gate)), sems)
    for h in range(2):
        ext[h, 0:PAD, :] = grad[h, rows - PAD :, :]
        ext[h, PAD : 2 * PAD, :] = after[h]
    for load in loads:
        load.wait()
    if count > PAD:
        glu_grad_rows(grad, rows - count, taps, value, gate, out_value, out_gate, 0, count - PAD)
    glu_grad_rows(ext, 0, taps, value, gate, out_value, out_gate, count - PAD, PAD)
    for copy in moves(((out_value, value_grad.at[at]), (out_gate, gate_grad.at[at])), sems):
        copy.wait()


def act_body(out_grad, weight, act):
    act[...] = lax.dot_general(out_grad[...], weight[...], NT, preferred_element_type=F32)


def proj_body(me, activ, out_grad, kept, sent):
    width = activ.shape[1]
    half = width // 2
    row = lax.broadcasted_iota(jnp.int32, (width, width), 0)
    col = lax.broadcasted_iota(jnp.int32, (width, width), 1)
    low = jnp.bitwise_and(row, half - 1)
    high = jnp.bitwise_xor(jnp.right_shift(row, 7), me[0])
    source = jnp.left_shift(jnp.right_shift(low, 1), 2) + 2 * high + jnp.bitwise_and(row, 1)
    order = (col == source).astype(F32).astype(BF16)
    placed = lax.dot_general(order, activ[...], NT, preferred_element_type=F32).astype(BF16)
    kept[...] = jnp.dot(placed[:half], out_grad[...], preferred_element_type=F32)
    sent[0:half] = jnp.dot(placed[half:], out_grad[...], preferred_element_type=F32)


def over_tp(array):
    return lax.all_to_all(array, "tp", 0, 0, tiled=True, axis_index_groups=[X_ORDER])


def per_device(glu_value, glu_gate, conv_taps, channel_gain, proj_weight, out_grad):
    n = conv_taps.shape[0]
    rows, width = glu_value.shape
    peers = lax.axis_size("tp")
    outs = out_grad.shape[1]
    factor = 1.0 / math.sqrt(rows * lax.axis_size(SP))

    def wide(length):
        return ((2, length, LANES), F32, "near")

    stat = ((peers, 2, rows), F32, "near")
    dma = pltpu.SemaphoreType.DMA
    tall = ((rows, width), BF16)
    glu, edge, taps = kernel(
        glu_body,
        [wide(rows + PAD), wide(PAD), ((n, width), F32, "near")],
        (far(glu_value), far(glu_gate), far(conv_taps)),
        ins=[HBM] * 3,
        scratch=[tall, tall, dma((2, 5))],
    )
    edge = shifted(edge, 1)
    conv, stats, out_grad, weight = kernel(
        conv_body,
        [
            wide(rows),
            ((8, rows), F32, "near"),
            (out_grad.shape, BF16, "near"),
            (proj_weight.shape, BF16, "near"),
        ],
        (far(out_grad), far(proj_weight), near(glu), near(taps)),
        ins=[HBM] * 2,
        scratch=[dma((2,))],
    )
    (act_grad,) = kernel(act_body, [((rows, width), F32, "near")], (near(out_grad), near(weight)))
    me = lax.axis_index("core")[None]
    edge, act_grad, me = lax.optimization_barrier((edge, act_grad, me))
    glu, conv, stats = kernel(
        head_body,
        [wide(rows + PAD), wide(rows), stat],
        (near(edge), near(glu), near(taps), near(conv), near(stats)),
        aliases={1: 0, 3: 1},
        scratch=[((8, 256), F32)],
    )
    stats = over_tp(stats)
    spreading = [((2, rows), F32), ((LANES, LANES), F32), ((2, rows, LANES), F32)]
    activ, xhat, scaled, sums, gain_sum = kernel(
        norm_body,
        [(*tall, "near"), wide(rows), wide(rows), stat, wide(8)],
        (near(stats), near(conv), near(act_grad), channel_gain[None]),
        scratch=spreading,
    )
    sums = over_tp(sums)
    sums, activ = lax.optimization_barrier((sums, activ))
    joint = ((width // 2 + 8, outs), F32, "near")
    kept, sent = kernel(
        proj_body,
        [((width // 2, outs), F32, "near"), joint],
        (me, near(activ), near(out_grad)),
        ins=[SMEM],
    )
    grad, sent = kernel(
        lambda *refs: taps_body(n, *refs),
        [wide(rows), joint],
        (near(sent), near(sums), near(scaled), near(xhat), near(glu), near(gain_sum)),
        aliases={0: 1},
        scratch=[*spreading, ((32, width), F32)],
    )
    received = swapped(sent)
    (first,) = kernel(
        pack_body, [((8, 16, outs + 512), BF16, "any")], (near(kept), near(sent), near(received))
    )
    first = lax.all_to_all(first, "z", 0, 0, tiled=True, axis_index_groups=[Z_ORDER])
    after = shifted(grad[:, :PAD], -1)

    def gates(length):
        return [((length, width), BF16)] * 4

    value_grad, gate_grad = kernel(
        glu_head_body,
        [(*tall, "far")] * 2,
        (far(glu_value), far(glu_gate), near(grad), conv_taps),
        ins=[HBM] * 2,
        out_specs=[HBM] * 2,
        scratch=[*gates(rows // 2), dma((2,))],
    )
    first, after, value_grad, gate_grad = lax.optimization_barrier((first, after, value_grad, gate_grad))
    (second,) = kernel(
        relay_body, [((8, 8, 1280), F32, "any")], (near(first),), scratch=[((16, outs), F32)]
    )
    second = lax.all_to_all(second, "y", 0, 0, tiled=True, axis_index_groups=[Y_ORDER])
    value_grad, gate_grad = kernel(
        glu_tail_body,
        [(*tall, "far")] * 2,
        (
            far(glu_value), far(glu_gate), far(value_grad), far(gate_grad), near(grad),
            near(after), conv_taps,
        ),
        ins=[HBM] * 4,
        out_specs=[HBM] * 2,
        aliases={2: 0, 3: 1},
        scratch=[*gates(rows // 2), ((2, 2 * PAD, LANES), F32), dma((2,))],
    )
    second, value_grad, gate_grad = lax.optimization_barrier((second, value_grad, gate_grad))
    proj_grad, taps_grad, gain_grad = kernel(
        lambda *refs: final_body(factor, *refs),
        [((2, outs), F32, "any"), ((n, width), F32, "any"), ((1, width), F32, "any")],
        (near(second),),
    )
    return (value_grad, gate_grad, proj_grad, taps_grad, gain_grad.reshape(width))


def solution(mesh):
    finer = Mesh(mesh.devices.reshape(8, 8, 2, mesh.shape["tp"]), (*SP, "tp"))
    return jax.shard_map(
        per_device,
        mesh=finer,
        in_specs=(P(SP, "tp"), P(SP, "tp"), P(None, "tp"), P("tp"), P("tp", None), P(SP, None)),
        out_specs=(P(SP, "tp"), P(SP, "tp"), P(("tp", *SP), None), P(None, "tp"), P("tp")),
        check_vma=False,
    )
```
